32 devices in a mesh: grp: 2 (over x), tp: 4 (over z), dp: 4 (over y, core).
Axes of the slice: x: 2, y: 2, z: 4, core: 2. Of those that a mesh axis runs over, the one named last changes fastest.
Arguments:
- tokens: bfloat16 [32, 4096], P(('grp', 'tp'), 'dp'), parts along dimension 0, may hold values from -30 to 30
- norm_gain: float32 [2, 4096], P(None, 'dp'), may hold values from 0.1 to 1.9
- w_query: bfloat16 [2, 4096, 2048], P(None, 'dp', 'tp'), may hold values from -0.09375 to 0.09375
- w_forget: bfloat16 [2, 4096, 2048], P(None, 'dp', 'tp'), may hold values from -0.09375 to 0.09375
- w_value: bfloat16 [2, 4096, 2048], P(None, 'dp', 'tp'), may hold values from -0.09375 to 0.09375
- w_gate: bfloat16 [2, 4096, 2048], P(None, 'dp', 'tp'), may hold values from -0.09375 to 0.09375
- lower_bound: float32 [2, 2048], P(None, 'tp'), may hold values from 0 to 0.9
- head_gain: float32 [2, 128], replicated, may hold values from 0.1 to 1.9
- w_out: bfloat16 [2, 2048, 4096], P(None, 'tp', 'dp'), may hold values from -0.125 to 0.125
- state: float32 [2, 32, 16, 128, 128], P(None, ('grp', 'dp'), 'tp'), parts along dimension 1, may hold values from -4 to 4
Outputs:
- hidden_out: bfloat16 [32, 4096], P(('grp', 'tp'), 'dp'), parts along dimension 0
- new_state: float32 [2, 32, 16, 128, 128], P(None, ('grp', 'dp'), 'tp'), parts along dimension 1
The draws below stay inside these ranges and needn't reach their ends.
There are 2 independent parts, one for each index of `grp`. The reference program is written for one: setup_inputs(seed, part) draws one part's arguments, and reference() takes and returns one part's arrays. A program takes and returns all parts, laid end to end along the dimension named above; an argument that names none is the same for every part. Nothing has to cross between parts.
All inputs are finite; a program needn't handle non-finite values.
Results may differ from the reference program's by a relative error of at most 0.02.
Values may be sent and summed in bfloat16 or wider, within the bound.
No kernel may reach another device: no remote copies, remote signals or barrier semaphores. Data moves between devices by JAX's collectives and lax.ppermute only.
A program may use at most 64 MiB of HBM per device.

```python
import jax
import jax.numpy as jnp
from jax import lax

D = 4096
HEADS = 16
HD = 128
DH = 2048
BATCH = 16


def draw_tokens(key, part):
    first_key, second_key = jax.random.split(key, 2)
    column_scale = jnp.repeat(jnp.exp(jax.random.uniform(second_key, (D // 16,), jnp.float32, -1.2, 1.2)), 16)
    values = jax.random.normal(first_key, (BATCH, D), jnp.float32) * column_scale
    return jnp.clip(values, -30.0, 30.0).astype(jnp.bfloat16)


def block_scale(own_key, extent, cuts, low, top_value):
    def one(position, blocks):
        steps = jax.random.uniform(jax.random.fold_in(jax.random.fold_in(own_key, 6), position), (blocks,), jnp.float32, low / len(cuts), top_value / len(cuts))
        return jnp.repeat(jnp.exp(steps), extent[position] // blocks).reshape((-1,) + (1,) * (len(extent) - position - 1))

    level = one(*cuts[0])
    for cut in cuts[1:]:
        level = level * one(*cut)
    return level


def centred(key, dims, width, most, cuts=(), dtype=jnp.bfloat16):
    level = block_scale(key, dims, cuts, -0.22, 0.18) if cuts else 1.0
    values = jax.random.normal(key, dims, jnp.float32) * width * level
    return jnp.minimum(jnp.maximum(values, -most), most).astype(dtype)


def setup_inputs(seed: int = 0, part: int = 0) -> dict:
    key_of = jax.random.split(jax.random.key(seed), 11)
    own_keys = jax.random.split(jax.random.fold_in(key_of[10], part), 11)
    return {
        "tokens": draw_tokens(jax.random.fold_in(jax.random.fold_in(key_of[10], part), 71), part),
        "norm_gain": jnp.clip(1.0 + 0.18 * jax.random.normal(key_of[1], (2, D), jnp.float32), 0.1, 1.9),
        "w_query": centred(key_of[2], (2, D, DH), D ** -0.5, 0.09375, ((1, 4), (2, 4))),
        "w_forget": centred(key_of[3], (2, D, DH), D ** -0.5, 0.09375, ((1, 4), (2, 4))),
        "w_value": centred(key_of[4], (2, D, DH), D ** -0.5, 0.09375, ((1, 4), (2, 4))),
        "w_gate": centred(key_of[5], (2, D, DH), D ** -0.5, 0.09375, ((1, 4), (2, 4))),
        "lower_bound": jnp.clip(0.9 * jax.random.uniform(key_of[6], (2, DH), jnp.float32) ** block_scale(key_of[6], (2, DH), ((1, 4),), -0.2, 0.2), 0.0, 0.9),
        "head_gain": jnp.clip(1.0 + 0.18 * jax.random.normal(key_of[7], (2, HD), jnp.float32), 0.1, 1.9),
        "w_out": centred(key_of[8], (2, DH, D), DH ** -0.5, 0.125, ((1, 4), (2, 4))),
        "state": centred(own_keys[9], (2, BATCH, HEADS, HD, HD), 0.5, 4.0, ((1, 4), (2, 4)), jnp.float32),
    }


def reference(tokens, norm_gain, w_query, w_forget, w_value, w_gate, lower_bound, head_gain, w_out, state):
    hidden = tokens
    updated = []
    for layer in range(2):
        widened = hidden.astype(jnp.float32)
        factor = lax.rsqrt(lax.optimization_barrier(jnp.mean(widened * widened, axis=1, keepdims=True)) + 1e-06)
        scaled = (widened * norm_gain[layer]).astype(jnp.bfloat16)
        query = jnp.dot(scaled, w_query[layer], preferred_element_type=jnp.float32) * factor
        forget_pre = jnp.dot(scaled, w_forget[layer], preferred_element_type=jnp.float32) * factor
        value = jnp.dot(scaled, w_value[layer], preferred_element_type=jnp.float32) * factor
        gate_pre = jnp.dot(scaled, w_gate[layer], preferred_element_type=jnp.float32) * factor
        bound = lower_bound[layer]
        forget = bound + (1.0 - bound) * jax.nn.sigmoid(forget_pre)
        keyvec = (1.0 - bound) * jax.nn.sigmoid(-forget_pre)
        count = hidden.shape[0]
        head_count = query.shape[1] // HD
        shaped = lambda arr: arr.reshape(count, head_count, HD)
        carried = shaped(forget)[..., None] * state[layer] + shaped(keyvec)[..., None] * shaped(value)[..., None, :]
        updated.append(carried)
        readout = jnp.einsum('bhkv,bhk->bhv', carried, shaped(query))
        readout = readout * lax.rsqrt(lax.optimization_barrier(jnp.mean(readout * readout, axis=-1, keepdims=True)) + 1e-06) * head_gain[layer]
        normed = (readout.reshape(count, head_count * HD) * jax.nn.sigmoid(gate_pre)).astype(jnp.bfloat16)
        mixed = jnp.dot(normed, w_out[layer], preferred_element_type=jnp.float32)
        hidden = (widened + mixed).astype(jnp.bfloat16)
    return (hidden, jnp.stack(updated))
```

```python
import jax
import jax.numpy as jnp
from jax import lax
from jax.sharding import PartitionSpec as P


def partners(n):
    if n & (n - 1) == 0:
        return [[i ^ k for i in range(n)] for k in range(n)]
    return [[(k - i) % n for i in range(n)] for k in range(n)]


def peer_of(n, k, index):
    if n & (n - 1) == 0:
        return jnp.bitwise_xor(index, k)
    return lax.rem(k - index + n, n)


def swap(array, axis, n, k):
    return lax.ppermute(array, axis, list(enumerate(partners(n)[k])))


def per_device(
    features,
    n_tp,
    n_dp,
    tokens,
    norm_gain,
    w_query,
    w_forget,
    w_value,
    w_gate,
    lower_bound,
    head_gain,
    w_out,
    state,
):
    seqs, heads, hd = state.shape[1], state.shape[2], state.shape[3]
    rows = tokens.shape[0]
    total = rows * n_tp
    tp = lax.axis_index("tp")
    dp = lax.axis_index("dp")

    def gather(array, axis, n, index):
        count = array.shape[0]
        out = jnp.zeros((count * n,) + array.shape[1:], array.dtype)
        parts = [array] + [swap(array, axis, n, k) for k in range(1, n)]
        for k, part in enumerate(parts):
            out = lax.dynamic_update_slice_in_dim(out, part, peer_of(n, k, index) * count, 0)
        return out

    def scatter_sum(array, axis, n, index):
        count = array.shape[0] // n
        own = lax.dynamic_slice_in_dim(array, index * count, count, 0)
        for k in range(1, n):
            piece = lax.dynamic_slice_in_dim(array, peer_of(n, k, index) * count, count, 0)
            own = own + swap(piece.astype(jnp.bfloat16), axis, n, k).astype(jnp.float32)
        return own

    hidden = gather(tokens, "tp", n_tp, tp)
    updated = []
    for layer in range(2):
        widened = hidden.astype(jnp.float32)
        squares = jnp.sum(widened * widened, axis=1, keepdims=True)
        scaled = (widened * norm_gain[layer]).astype(jnp.bfloat16)
        high = squares.astype(jnp.bfloat16).astype(jnp.float32)
        middle = (squares - high).astype(jnp.bfloat16).astype(jnp.float32)
        low = squares - high - middle
        joined = jnp.concatenate(
            [
                jnp.dot(scaled, weight[layer], preferred_element_type=jnp.float32)
                for weight in (w_query, w_forget, w_value, w_gate)
            ]
            + [jnp.concatenate([high, middle, low, jnp.zeros((total, 125), jnp.float32)], axis=1)],
            axis=1,
        )
        own = scatter_sum(joined, "dp", n_dp, dp)
        width = heads * hd
        mean = jnp.sum(own[:, 4 * width :], axis=1, keepdims=True) / features
        factor = lax.rsqrt(mean + 1e-06)
        query, forget_pre, value, gate_pre = (
            own[:, index * width : (index + 1) * width] * factor for index in range(4)
        )
        bound = lower_bound[layer]
        forget = bound + (1.0 - bound) * jax.nn.sigmoid(forget_pre)
        keyvec = (1.0 - bound) * jax.nn.sigmoid(-forget_pre)

        def shaped(array):
            return array.reshape(seqs, heads, hd)

        carried = (
            shaped(forget)[..., None] * state[layer]
            + shaped(keyvec)[..., None] * shaped(value)[..., None, :]
        )
        updated.append(carried)
        readout = jnp.einsum("bhkv,bhk->bhv", carried, shaped(query))
        readout = (
            readout
            * lax.rsqrt(jnp.mean(readout * readout, axis=-1, keepdims=True) + 1e-06)
            * head_gain[layer]
        )
        normed = (readout.reshape(seqs, width) * jax.nn.sigmoid(gate_pre)).astype(jnp.bfloat16)
        mixed = jnp.dot(
            gather(normed, "dp", n_dp, dp), w_out[layer], preferred_element_type=jnp.float32
        )
        if layer == 0:
            sent = mixed.astype(jnp.bfloat16)
            for k in range(1, n_tp):
                mixed = mixed + swap(sent, "tp", n_tp, k).astype(jnp.float32)
            hidden = (widened + mixed).astype(jnp.bfloat16)
        else:
            base = lax.dynamic_slice_in_dim(widened, tp * rows, rows, 0)
            hidden = (base + scatter_sum(mixed, "tp", n_tp, tp)).astype(jnp.bfloat16)
    return (hidden, jnp.stack(updated))


def solution(mesh):
    n_tp, n_dp = mesh.shape["tp"], mesh.shape["dp"]

    def body(tokens, *rest):
        return per_device(tokens.shape[1] * n_dp, n_tp, n_dp, tokens, *rest)

    return jax.shard_map(
        body,
        mesh=mesh,
        in_specs=(
            P(("grp", "tp"), "dp"),
            P(None, "dp"),
            P(None, "dp", "tp"),
            P(None, "dp", "tp"),
            P(None, "dp", "tp"),
            P(None, "dp", "tp"),
            P(None, "tp"),
            P(),
            P(None, "tp", "dp"),
            P(None, ("grp", "dp"), "tp", None, None),
        ),
        out_specs=(P(("grp", "tp"), "dp"), P(None, ("grp", "dp"), "tp", None, None)),
        check_vma=False,
    )
```

```python
import functools

import jax
import jax.numpy as jnp
from jax import lax
from jax.experimental import pallas as pl
from jax.experimental.pallas import tpu as pltpu
from jax.sharding import PartitionSpec as P

F32, BF16 = jnp.float32, jnp.bfloat16
LANES = 128
VMEM = pl.BlockSpec(memory_space=pltpu.VMEM)
ANY = pl.BlockSpec(memory_space=pl.ANY)


def peer_of(n, k, index):
    if n & (n - 1) == 0:
        return index ^ k
    return (index + k) % n


def swap(array, axis, n, k):
    return lax.ppermute(array, axis, [(peer_of(n, k, i), i) for i in range(n)])


def send(array, axis, n, k):
    return lax.ppermute(array, axis, [(i, peer_of(n, k, i)) for i in range(n)])


def slot_rows(total, n, index):
    size = total // n
    row = jnp.arange(total, dtype=jnp.int32)
    return peer_of(n, row // size, index) * size + row % size


def split(array):
    high = array.astype(BF16)
    return high, (array - high.astype(F32)).astype(BF16)


def finish_projection(base, gain_ref, layer, weights, outs):
    count = outs[0].shape[0]
    squares = jnp.sum(base * base, axis=1, keepdims=True)
    scaled = (base * gain_ref[layer : layer + 1, :]).astype(BF16)
    high, rest = split(squares)
    high = high.astype(F32)
    middle, low = split(squares - high)
    lane = lax.broadcasted_iota(jnp.int32, (base.shape[0], LANES), 1)
    zero = jnp.zeros((base.shape[0], LANES), F32)
    tail = jnp.where(lane == 0, high, zero)
    tail = jnp.where(lane == 1, middle.astype(F32), tail)
    tail = jnp.where(lane == 2, low.astype(F32), tail)
    width = weights[0].shape[-1]
    for index, weight in enumerate(weights):
        product = jnp.dot(scaled, weight[0], preferred_element_type=F32)
        for k, out in enumerate(outs):
            out[:, index * width : (index + 1) * width] = product[
                k * count : (k + 1) * count
            ].astype(out.dtype)
    for k, out in enumerate(outs):
        out[:, 4 * width :] = tail[k * count : (k + 1) * count].astype(out.dtype)


def project_first(n_tp, n_dp, layer, *refs):
    parts, (order, gain), weights = refs[:n_tp], refs[n_tp : n_tp + 2], refs[n_tp + 2 : n_tp + 6]
    base_out, outs, slots = refs[n_tp + 6], refs[n_tp + 7 : -1], refs[-1]
    rows = parts[0].shape[0]
    for k, part in enumerate(parts):
        slots[k * rows : (k + 1) * rows, :] = part[...].astype(F32)
    base = jnp.dot(order[...], slots[...].astype(BF16), preferred_element_type=F32)
    base_out[...] = base.astype(BF16)
    finish_projection(base, gain, layer, weights, outs)


def project_next(n_tp, n_dp, layer, *refs):
    (base_in, mixed), parts = refs[:2], refs[2 : n_tp + 1]
    gain, weights = refs[n_tp + 1], refs[n_tp + 2 : n_tp + 6]
    base_out, outs = refs[n_tp + 6], refs[n_tp + 7 :]
    base = base_in[...].astype(F32) + mixed[...]
    for part in parts:
        base = base + part[...].astype(F32)
    rounded = base.astype(BF16)
    base_out[...] = rounded
    finish_projection(rounded.astype(F32), gain, layer, weights, outs)


def recur(n_dp, layer, features, *refs):
    own, parts = refs[0], refs[1:n_dp]
    bound_ref, head_gain, state, normed, gates = refs[n_dp:]
    seqs, heads, hd = state.shape[1], state.shape[2], state.shape[3]
    width = heads * hd
    total = own[...]
    for part in parts:
        total = total + part[...].astype(F32)
    mean = jnp.sum(total[:, 4 * width :], axis=1, keepdims=True) / features
    factor = lax.rsqrt(mean + 1e-06)
    query, forget_pre, value, gate_pre = (
        total[:, index * width : (index + 1) * width] * factor for index in range(4)
    )
    bound = bound_ref[layer : layer + 1, :]
    forget = bound + (1.0 - bound) * jax.nn.sigmoid(forget_pre)
    keyvec = (1.0 - bound) * jax.nn.sigmoid(-forget_pre)
    for seq in range(seqs):
        for index, vector in enumerate((forget, keyvec, value)):
            gates[seq, index : index + 1, :] = vector[seq : seq + 1]
    gate = jax.nn.sigmoid(gate_pre)
    weighted = query * forget
    shared = query * keyvec
    row = lax.broadcasted_iota(jnp.int32, (seqs, hd), 0)
    for head in range(heads):
        cols = slice(head * hd, (head + 1) * hd)
        readout = jnp.sum(shared[:, cols], axis=1, keepdims=True) * value[:, cols]
        for seq in range(seqs):
            high, low = split(jnp.where(row == seq, weighted[:, cols], 0.0))
            stored = state[0, seq, head].astype(BF16)
            readout = readout + jnp.dot(high, stored, preferred_element_type=F32)
            readout = readout + jnp.dot(low, stored, preferred_element_type=F32)
        scale = lax.rsqrt(jnp.mean(readout * readout, axis=1, keepdims=True) + 1e-06)
        normed[:, cols] = (
            readout * scale * head_gain[layer : layer + 1, :] * gate[:, cols]
        ).astype(BF16)


def update(gates, state, *refs):
    out = refs[-1]
    heads, hd = state.shape[2], state.shape[3]
    for head in range(heads):
        cols = slice(head * hd, (head + 1) * hd)
        forget, keyvec, value = (gates[0, index : index + 1, cols] for index in range(3))
        forget = jnp.transpose(jnp.broadcast_to(forget, (hd, hd)))
        keyvec = jnp.transpose(jnp.broadcast_to(keyvec, (hd, hd)))
        out[0, 0, head] = forget * state[0, 0, head] + keyvec * value


def gather_rows(parts, slots):
    rows = parts[0].shape[0]
    for k, part in enumerate(parts):
        slots[k * rows : (k + 1) * rows, :] = part[...].astype(F32)
    return slots[...].astype(BF16)


def mix_next(n_dp, *refs):
    parts, (weight, mixed, sent, slots) = refs[:n_dp], refs[n_dp:]
    product = jnp.dot(gather_rows(parts, slots), weight[0], preferred_element_type=F32)
    mixed[...] = product
    sent[...] = product.astype(BF16)


def mix_last(n_dp, *refs):
    parts, (weight, base, order) = refs[:n_dp], refs[n_dp : n_dp + 3]
    own, outs, slots = refs[n_dp + 3], refs[n_dp + 4 : -1], refs[-1]
    rows = own.shape[0]
    product = jnp.dot(gather_rows(parts, slots), weight[0], preferred_element_type=F32)
    high, low = split(product)
    moved = jnp.dot(order[...], high, preferred_element_type=F32)
    first = order[:rows, :]
    own[...] = (
        moved[:rows]
        + jnp.dot(first, low, preferred_element_type=F32)
        + jnp.dot(first, base[...], preferred_element_type=F32)
    )
    for k, out in enumerate(outs):
        out[...] = moved[(k + 1) * rows : (k + 2) * rows].astype(BF16)


def close(own, *refs):
    total = own[...]
    for part in refs[:-1]:
        total = total + part[...].astype(F32)
    refs[-1][...] = total.astype(BF16)


def layer_block(array, layer):
    zeros = (0,) * (array.ndim - 1)
    return pl.BlockSpec((1,) + array.shape[1:], lambda step: (layer,) + zeros)


def call(body, name, args, in_specs, outs, scratch=()):
    return pl.pallas_call(
        body,
        name=name,
        grid=(1,),
        out_shape=[jax.ShapeDtypeStruct(shape, dtype) for shape, dtype in outs],
        in_specs=in_specs,
        out_specs=[VMEM] * len(outs),
        scratch_shapes=[pltpu.VMEM(shape, dtype) for shape, dtype in scratch],
    )(*args)


def per_device(
    n_tp,
    n_dp,
    tokens,
    norm_gain,
    w_query,
    w_forget,
    w_value,
    w_gate,
    lower_bound,
    head_gain,
    w_out,
    state,
):
    seqs, heads, hd = state.shape[1], state.shape[2], state.shape[3]
    rows, local = tokens.shape
    features = local * n_dp
    total = rows * n_tp
    width = heads * hd
    weights = (w_query, w_forget, w_value, w_gate)
    tp_rows = slot_rows(total, n_tp, lax.axis_index("tp"))
    dp_rows = slot_rows(total, n_dp, lax.axis_index("dp"))
    order_in = (dp_rows[:, None] == tp_rows[None, :]).astype(BF16)
    order_out = (tp_rows[:, None] == dp_rows[None, :]).astype(BF16)

    parts = [tokens] + [swap(tokens, "tp", n_tp, k) for k in range(1, n_tp)]
    base = mixed = None
    new_state = None
    for layer in range(2):
        outs = [((total, local), BF16), ((seqs, 4 * width + LANES), F32)]
        outs += [((seqs, 4 * width + LANES), BF16)] * (n_dp - 1)
        specs = [layer_block(weight, layer) for weight in weights]
        if layer == 0:
            base, own, *sent = call(
                functools.partial(project_first, n_tp, n_dp, layer),
                "project_first",
                (*parts, order_in, norm_gain, *weights),
                [VMEM] * (n_tp + 2) + specs,
                outs,
                [((total, local), F32)],
            )
        else:
            base, own, *sent = call(
                functools.partial(project_next, n_tp, n_dp, layer),
                "project_next",
                (base, mixed, *parts, norm_gain, *weights),
                [VMEM] * (n_tp + 2) + specs,
                outs,
            )
        parts = [send(sent[k - 1], "dp", n_dp, k) for k in range(1, n_dp)]
        normed, gates = call(
            functools.partial(recur, n_dp, layer, features),
            "recur",
            (own, *parts, lower_bound, head_gain, state),
            [VMEM] * (n_dp + 2) + [layer_block(state, layer)],
            [((seqs, width), BF16), ((seqs, 3, width), F32)],
        )
        parts = [normed] + [swap(normed, "dp", n_dp, k) for k in range(1, n_dp)]
        block = pl.BlockSpec(
            (1, 1, heads, hd, hd), lambda seq, layer=layer: (layer, seq, 0, 0, 0)
        )
        gate_block = pl.BlockSpec((1, 3, width), lambda seq: (seq, 0, 0))
        new_state = pl.pallas_call(
            update,
            name="update",
            grid=(seqs,),
            out_shape=jax.ShapeDtypeStruct(state.shape, F32),
            in_specs=[gate_block, block] + ([ANY] if layer else []),
            out_specs=block,
            input_output_aliases={2: 0} if layer else {},
        )(gates, state, *((new_state,) if layer else ()))
        if layer == 0:
            mixed, sent = call(
                functools.partial(mix_next, n_dp),
                "mix_next",
                (*parts, w_out),
                [VMEM] * n_dp + [layer_block(w_out, layer)],
                [((total, local), F32), ((total, local), BF16)],
                [((total, width), F32)],
            )
            parts = [swap(sent, "tp", n_tp, k) for k in range(1, n_tp)]
        else:
            own, *sent = call(
                functools.partial(mix_last, n_dp),
                "mix_last",
                (*parts, w_out, base, order_out),
                [VMEM] * n_dp + [layer_block(w_out, layer)] + [VMEM] * 2,
                [((rows, local), F32)] + [((rows, local), BF16)] * (n_tp - 1),
                [((total, width), F32)],
            )
            parts = [send(sent[k - 1], "tp", n_tp, k) for k in range(1, n_tp)]
    (hidden,) = call(
        close, "close", (own, *parts), [VMEM] * n_tp, [((rows, local), BF16)]
    )
    return (hidden, new_state)


def solution(mesh):
    n_tp, n_dp = mesh.shape["tp"], mesh.shape["dp"]
    return jax.shard_map(
        functools.partial(per_device, n_tp, n_dp),
        mesh=mesh,
        in_specs=(
            P(("grp", "tp"), "dp"),
            P(None, "dp"),
            P(None, "dp", "tp"),
            P(None, "dp", "tp"),
            P(None, "dp", "tp"),
            P(None, "dp", "tp"),
            P(None, "tp"),
            P(),
            P(None, "tp", "dp"),
            P(None, ("grp", "dp"), "tp", None, None),
        ),
        out_specs=(P(("grp", "tp"), "dp"), P(None, ("grp", "dp"), "tp", None, None)),
        check_vma=False,
    )
```

```python
import functools

import jax
import jax.numpy as jnp
from jax import lax
from jax.experimental import pallas as pl
from jax.experimental.pallas import tpu as pltpu
from jax.sharding import PartitionSpec as P

F32, BF16 = jnp.float32, jnp.bfloat16
LANES = 128
VMEM = pl.BlockSpec(memory_space=pltpu.VMEM)
ANY = pl.BlockSpec(memory_space=pl.ANY)


def peer_of(n, k, index):
    if n & (n - 1) == 0:
        return index ^ k
    return (index + k) % n


def swap(array, axis, n, k):
    return lax.ppermute(array, axis, [(peer_of(n, k, i), i) for i in range(n)])


def send(array, axis, n, k):
    return lax.ppermute(array, axis, [(i, peer_of(n, k, i)) for i in range(n)])


def split(array):
    high = array.astype(BF16)
    return high, (array - high.astype(F32)).astype(BF16)


def finish_projection(base, gain_ref, layer, weights, outs):
    count = outs[0].shape[0]
    squares = jnp.sum(base * base, axis=1, keepdims=True)
    scaled = (base * gain_ref[layer : layer + 1, :]).astype(BF16)
    high, rest = split(squares)
    high = high.astype(F32)
    middle, low = split(squares - high)
    lane = lax.broadcasted_iota(jnp.int32, (base.shape[0], LANES), 1)
    zero = jnp.zeros((base.shape[0], LANES), F32)
    tail = jnp.where(lane == 0, high, zero)
    tail = jnp.where(lane == 1, middle.astype(F32), tail)
    tail = jnp.where(lane == 2, low.astype(F32), tail)
    width = weights[0].shape[-1]
    for index, weight in enumerate(weights):
        product = jnp.dot(scaled, weight[layer], preferred_element_type=F32)
        for k, out in enumerate(outs):
            out[:, index * width : (index + 1) * width] = product[
                k * count : (k + 1) * count
            ].astype(out.dtype)
    for k, out in enumerate(outs):
        out[:, 4 * width :] = tail[k * count : (k + 1) * count].astype(out.dtype)


def project_first(n_tp, n_dp, layer, *refs):
    parts, (order, gain), weights = refs[:n_tp], refs[n_tp : n_tp + 2], refs[n_tp + 2 : n_tp + 6]
    base_out, outs, slots = refs[n_tp + 6], refs[n_tp + 7 : -1], refs[-1]
    rows = parts[0].shape[0]
    for k, part in enumerate(parts):
        slots[k * rows : (k + 1) * rows, :] = part[...].astype(F32)
    base = jnp.dot(order[...], slots[...].astype(BF16), preferred_element_type=F32)
    base_out[...] = base.astype(BF16)
    finish_projection(base, gain, layer, weights, outs)


def project_next(n_tp, n_dp, layer, *refs):
    (base_in, mixed), parts = refs[:2], refs[2 : n_tp + 1]
    gain, weights = refs[n_tp + 1], refs[n_tp + 2 : n_tp + 6]
    base_out, outs = refs[n_tp + 6], refs[n_tp + 7 :]
    base = base_in[...].astype(F32) + mixed[...]
    for part in parts:
        base = base + part[...].astype(F32)
    rounded = base.astype(BF16)
    base_out[...] = rounded
    finish_projection(rounded.astype(F32), gain, layer, weights, outs)


def recur(n_dp, layer, features, *refs):
    own, parts = refs[0], refs[1:n_dp]
    bound_ref, head_gain, state, normed, gates = refs[n_dp:]
    seqs, heads, hd = state.shape[1], state.shape[2], state.shape[3]
    width = heads * hd
    total = own[...]
    for part in parts:
        total = total + part[...].astype(F32)
    mean = jnp.sum(total[:, 4 * width :], axis=1, keepdims=True) / features
    factor = lax.rsqrt(mean + 1e-06)
    query, forget_pre, value, gate_pre = (
        total[:, index * width : (index + 1) * width] * factor for index in range(4)
    )
    bound = bound_ref[layer : layer + 1, :]
    forget = bound + (1.0 - bound) * jax.nn.sigmoid(forget_pre)
    keyvec = (1.0 - bound) * jax.nn.sigmoid(-forget_pre)
    for seq in range(seqs):
        for index, vector in enumerate((forget, keyvec, value)):
            gates[seq, index : index + 1, :] = vector[seq : seq + 1]
    gate = jax.nn.sigmoid(gate_pre)
    weighted = query * forget
    shared = query * keyvec
    row = lax.broadcasted_iota(jnp.int32, (seqs, hd), 0)
    for head in range(heads):
        cols = slice(head * hd, (head + 1) * hd)
        readout = jnp.sum(shared[:, cols], axis=1, keepdims=True) * value[:, cols]
        for seq in range(seqs):
            high, low = split(jnp.where(row == seq, weighted[:, cols], 0.0))
            stored = state[layer, seq, head].astype(BF16)
            readout = readout + jnp.dot(high, stored, preferred_element_type=F32)
            readout = readout + jnp.dot(low, stored, preferred_element_type=F32)
        scale = lax.rsqrt(jnp.mean(readout * readout, axis=1, keepdims=True) + 1e-06)
        normed[:, cols] = (
            readout * scale * head_gain[layer : layer + 1, :] * gate[:, cols]
        ).astype(BF16)


def update(layer, gates, state, *refs):
    out, staged, sems = refs[-3:]
    seqs, heads, hd = state.shape[1], state.shape[2], state.shape[3]
    copies = []
    for seq in range(seqs):
        for head in range(heads):
            cols = slice(head * hd, (head + 1) * hd)
            forget, keyvec, value = (gates[seq, index : index + 1, cols] for index in range(3))
            forget = jnp.transpose(jnp.broadcast_to(forget, (hd, hd)))
            keyvec = jnp.transpose(jnp.broadcast_to(keyvec, (hd, hd)))
            staged[seq, head] = forget * state[layer, seq, head] + keyvec * value
        copies.append(pltpu.make_async_copy(staged.at[seq], out.at[layer, seq], sems.at[seq]))
        copies[-1].start()
    for copy in copies:
        copy.wait()


def gather_rows(parts, slots):
    rows = parts[0].shape[0]
    for k, part in enumerate(parts):
        slots[k * rows : (k + 1) * rows, :] = part[...].astype(F32)
    return slots[...].astype(BF16)


def mix_next(n_dp, layer, *refs):
    parts, (weight, mixed, sent, slots) = refs[:n_dp], refs[n_dp:]
    product = jnp.dot(gather_rows(parts, slots), weight[layer], preferred_element_type=F32)
    mixed[...] = product
    sent[...] = product.astype(BF16)


def mix_last(n_dp, layer, *refs):
    parts, (weight, base, order) = refs[:n_dp], refs[n_dp : n_dp + 3]
    own, outs, slots = refs[n_dp + 3], refs[n_dp + 4 : -1], refs[-1]
    rows = own.shape[0]
    product = jnp.dot(gather_rows(parts, slots), weight[layer], preferred_element_type=F32)
    high, low = split(product)
    moved = jnp.dot(order[...], high, preferred_element_type=F32)
    first = order[:rows, :]
    own[...] = (
        moved[:rows]
        + jnp.dot(first, low, preferred_element_type=F32)
        + jnp.dot(first, base[...], preferred_element_type=F32)
    )
    for k, out in enumerate(outs):
        out[...] = moved[(k + 1) * rows : (k + 2) * rows].astype(BF16)


def close(own, *refs):
    total = own[...]
    for part in refs[:-1]:
        total = total + part[...].astype(F32)
    refs[-1][...] = total.astype(BF16)


def in_vmem(array):
    return pltpu.with_memory_space_constraint(array, pltpu.VMEM)


def stage(n_tp, n_dp, tokens, tokens_out, order_in, order_out):
    tokens_out[...] = tokens[...]
    total = order_in.shape[0]

    def held(dim, n, index):
        row = lax.broadcasted_iota(jnp.int32, (total, total), dim)
        size = total // n
        return peer_of(n, row // size, index) * size + row % size

    tp, dp = lax.axis_index("tp"), lax.axis_index("dp")
    order_in[...] = jnp.where(held(0, n_dp, dp) == held(1, n_tp, tp), 1.0, 0.0).astype(BF16)
    order_out[...] = jnp.where(held(0, n_tp, tp) == held(1, n_dp, dp), 1.0, 0.0).astype(BF16)


def call(body, name, args, in_specs, outs, scratch=(), flops=None):
    return pl.pallas_call(
        body,
        name=name,
        out_shape=[pltpu.VMEM(shape, dtype) for shape, dtype in outs],
        in_specs=in_specs,
        out_specs=[VMEM] * len(outs),
        scratch_shapes=[pltpu.VMEM(shape, dtype) for shape, dtype in scratch],
        compiler_params=pltpu.CompilerParams(vmem_limit_bytes=8 << 20),
        cost_estimate=flops and pl.CostEstimate(flops=flops, bytes_accessed=0, transcendentals=0),
    )(*map(in_vmem, args))


def per_device(
    n_tp,
    n_dp,
    tokens,
    norm_gain,
    w_query,
    w_forget,
    w_value,
    w_gate,
    lower_bound,
    head_gain,
    w_out,
    state,
):
    seqs, heads, hd = state.shape[1], state.shape[2], state.shape[3]
    rows, local = tokens.shape
    features = local * n_dp
    total = rows * n_tp
    width = heads * hd
    weights = (w_query, w_forget, w_value, w_gate)
    tokens, order_in, order_out = call(
        functools.partial(stage, n_tp, n_dp),
        "stage",
        (tokens,),
        [VMEM],
        [((rows, local), BF16)] + [((total, total), BF16)] * 2,
        flops=20_000_000_000,
    )
    parts = [tokens] + [swap(tokens, "tp", n_tp, k) for k in range(1, n_tp)]
    base = mixed = None
    new_state = None
    for layer in range(2):
        outs = [((total, local), BF16), ((seqs, 4 * width + LANES), F32)]
        outs += [((seqs, 4 * width + LANES), BF16)] * (n_dp - 1)
        specs = [VMEM] * 4
        if layer == 0:
            base, own, *sent = call(
                functools.partial(project_first, n_tp, n_dp, layer),
                "project_first",
                (*parts, order_in, norm_gain, *weights),
                [VMEM] * (n_tp + 2) + specs,
                outs,
                [((total, local), F32)],
            )
        else:
            base, own, *sent = call(
                functools.partial(project_next, n_tp, n_dp, layer),
                "project_next",
                (base, mixed, *parts, norm_gain, *weights),
                [VMEM] * (n_tp + 2) + specs,
                outs,
            )
        parts = [send(sent[k - 1], "dp", n_dp, k) for k in range(1, n_dp)]
        normed, gates = call(
            functools.partial(recur, n_dp, layer, features),
            "recur",
            (own, *parts, lower_bound, head_gain, state),
            [VMEM] * (n_dp + 2) + [VMEM],
            [((seqs, width), BF16), ((seqs, 3, width), F32)],
        )
        parts = [normed] + [swap(normed, "dp", n_dp, k) for k in range(1, n_dp)]
        new_state = pl.pallas_call(
            functools.partial(update, layer),
            name="update",
            out_shape=jax.ShapeDtypeStruct(state.shape, F32),
            in_specs=[VMEM, VMEM] + ([ANY] if layer else []),
            out_specs=ANY,
            input_output_aliases={2: 0} if layer else {},
            scratch_shapes=[
                pltpu.VMEM((seqs, heads, hd, hd), F32),
                pltpu.SemaphoreType.DMA((seqs,)),
            ],
            compiler_params=pltpu.CompilerParams(vmem_limit_bytes=4 << 20),
        )(in_vmem(gates), in_vmem(state), *((new_state,) if layer else ()))
        if layer == 0:
            mixed, sent = call(
                functools.partial(mix_next, n_dp, layer),
                "mix_next",
                (*parts, w_out),
                [VMEM] * n_dp + [VMEM],
                [((total, local), F32), ((total, local), BF16)],
                [((total, width), F32)],
            )
            parts = [swap(sent, "tp", n_tp, k) for k in range(1, n_tp)]
        else:
            own, *sent = call(
                functools.partial(mix_last, n_dp, layer),
                "mix_last",
                (*parts, w_out, base, order_out),
                [VMEM] * n_dp + [VMEM] + [VMEM] * 2,
                [((rows, local), F32)] + [((rows, local), BF16)] * (n_tp - 1),
                [((total, width), F32)],
            )
            parts = [send(sent[k - 1], "tp", n_tp, k) for k in range(1, n_tp)]
    hidden = pl.pallas_call(
        close,
        name="close",
        out_shape=jax.ShapeDtypeStruct((rows, local), BF16),
        in_specs=[VMEM] * n_tp,
        out_specs=VMEM,
        compiler_params=pltpu.CompilerParams(vmem_limit_bytes=4 << 20),
    )(*map(in_vmem, (own, *parts)))
    return (hidden, new_state)


def solution(mesh):
    n_tp, n_dp = mesh.shape["tp"], mesh.shape["dp"]
    return jax.shard_map(
        functools.partial(per_device, n_tp, n_dp),
        mesh=mesh,
        in_specs=(
            P(("grp", "tp"), "dp"),
            P(None, "dp"),
            P(None, "dp", "tp"),
            P(None, "dp", "tp"),
            P(None, "dp", "tp"),
            P(None, "dp", "tp"),
            P(None, "tp"),
            P(),
            P(None, "tp", "dp"),
            P(None, ("grp", "dp"), "tp", None, None),
        ),
        out_specs=(P(("grp", "tp"), "dp"), P(None, ("grp", "dp"), "tp", None, None)),
        check_vma=False,
    )
```

```python
import functools

import jax
import jax.numpy as jnp
from jax import lax
from jax.experimental import pallas as pl
from jax.experimental.pallas import tpu as pltpu
from jax.sharding import PartitionSpec as P


F32, BF16 = jnp.float32, jnp.bfloat16
LANES = 128
VMEM = pl.BlockSpec(memory_space=pltpu.VMEM)
ANY = pl.BlockSpec(memory_space=pl.ANY)


def peer_of(n, k, index):
    if n & (n - 1) == 0:
        return index ^ k
    return (index + k) % n


def exchange(axis, n, arrays, inward=False):
    parts = [None] * (n - 1)
    for k in reversed(range(1, n)):
        pairs = [(i, peer_of(n, k, i)) for i in range(n)]
        parts[k - 1] = lax.ppermute(
            arrays[k - 1], axis, [(b, a) for a, b in pairs] if inward else pairs
        )
    return parts


def gather(axis, n, array):
    return [array] + exchange(axis, n, [array] * (n - 1), inward=True)


def split(array):
    high = array.astype(BF16)
    return high, (array - high.astype(F32)).astype(BF16)


def finish_projection(base, gain_ref, layer, weights, outs):
    count = outs[0].shape[0]
    squares = jnp.sum(base * base, axis=1, keepdims=True)
    scaled = (base * gain_ref[layer : layer + 1, :]).astype(BF16)
    high, _ = split(squares)
    high = high.astype(F32)
    middle, low = split(squares - high)
    lane = lax.broadcasted_iota(jnp.int32, (base.shape[0], LANES), 1)
    zero = jnp.zeros((base.shape[0], LANES), F32)
    tail = jnp.where(lane == 0, high, zero)
    tail = jnp.where(lane == 1, middle.astype(F32), tail)
    tail = jnp.where(lane == 2, low.astype(F32), tail)
    width = weights[0].shape[-1]
    for index, weight in enumerate(weights):
        product = jnp.dot(scaled, weight[layer], preferred_element_type=F32)
        for k, out in enumerate(outs):
            out[:, index * width : (index + 1) * width] = product[
                k * count : (k + 1) * count
            ].astype(out.dtype)
    for k, out in enumerate(outs):
        out[:, 4 * width :] = tail[k * count : (k + 1) * count].astype(out.dtype)


def project_first(n_tp, layer, *refs):
    parts, (order, gain), weights = refs[:n_tp], refs[n_tp : n_tp + 2], refs[n_tp + 2 : n_tp + 6]
    base_out, outs, slots = refs[n_tp + 6], refs[n_tp + 7 : -1], refs[-1]
    rows = parts[0].shape[0]
    for k, part in enumerate(parts):
        slots[k * rows : (k + 1) * rows, :] = part[...].astype(F32)
    base = jnp.dot(order[...], slots[...].astype(BF16), preferred_element_type=F32)
    base_out[...] = base.astype(BF16)
    finish_projection(base, gain, layer, weights, outs)


def project_next(n_tp, layer, *refs):
    (base_in, mixed), parts = refs[:2], refs[2 : n_tp + 1]
    gain, weights = refs[n_tp + 1], refs[n_tp + 2 : n_tp + 6]
    base_out, outs = refs[n_tp + 6], refs[n_tp + 7 :]
    base = base_in[...].astype(F32) + mixed[...]
    for part in parts:
        base = base + part[...].astype(F32)
    rounded = base.astype(BF16)
    base_out[...] = rounded
    finish_projection(rounded.astype(F32), gain, layer, weights, outs)


def recur(n_dp, layer, features, *refs):
    own, parts = refs[0], refs[1:n_dp]
    bound_ref, head_gain, state, normed, gates = refs[n_dp:]
    seqs, heads, hd = state.shape[1], state.shape[2], state.shape[3]
    width = heads * hd
    total = own[...]
    for part in parts:
        total = total + part[...].astype(F32)
    mean = jnp.sum(total[:, 4 * width :], axis=1, keepdims=True) / features
    factor = lax.rsqrt(mean + 1e-06)
    query, forget_pre, value, gate_pre = (
        total[:, index * width : (index + 1) * width] * factor for index in range(4)
    )
    bound = bound_ref[layer : layer + 1, :]
    forget = bound + (1.0 - bound) * jax.nn.sigmoid(forget_pre)
    keyvec = (1.0 - bound) * jax.nn.sigmoid(-forget_pre)
    for seq in range(seqs):
        for index, vector in enumerate((forget, keyvec, value)):
            gates[seq, index : index + 1, :] = vector[seq : seq + 1]
    gate = jax.nn.sigmoid(gate_pre)
    weighted = query * forget
    shared = query * keyvec
    row = lax.broadcasted_iota(jnp.int32, (seqs, hd), 0)
    for head in range(heads):
        cols = slice(head * hd, (head + 1) * hd)
        readout = jnp.sum(shared[:, cols], axis=1, keepdims=True) * value[:, cols]
        for seq in range(seqs):
            high, low = split(jnp.where(row == seq, weighted[:, cols], 0.0))
            stored = state[layer, seq, head].astype(BF16)
            readout = readout + jnp.dot(high, stored, preferred_element_type=F32)
            readout = readout + jnp.dot(low, stored, preferred_element_type=F32)
        scale = lax.rsqrt(jnp.mean(readout * readout, axis=1, keepdims=True) + 1e-06)
        normed[:, cols] = (
            readout * scale * head_gain[layer : layer + 1, :] * gate[:, cols]
        ).astype(BF16)


def update(layer, gates, state, *refs):
    out, staged, sems = refs[-3:]
    seqs, heads, hd = state.shape[1], state.shape[2], state.shape[3]
    copies = []
    for seq in range(seqs):
        for head in range(heads):
            cols = slice(head * hd, (head + 1) * hd)
            forget, keyvec, value = (gates[seq, index : index + 1, cols] for index in range(3))
            forget = jnp.transpose(jnp.broadcast_to(forget, (hd, hd)))
            keyvec = jnp.transpose(jnp.broadcast_to(keyvec, (hd, hd)))
            staged[seq, head] = forget * state[layer, seq, head] + keyvec * value
        copies.append(pltpu.make_async_copy(staged.at[seq], out.at[layer, seq], sems.at[seq]))
        copies[-1].start()
    for copy in copies:
        copy.wait()


def gather_rows(parts, slots):
    rows = parts[0].shape[0]
    for k, part in enumerate(parts):
        slots[k * rows : (k + 1) * rows, :] = part[...].astype(F32)
    return slots[...].astype(BF16)


def mix_next(n_dp, layer, *refs):
    parts, (weight, mixed, sent, slots) = refs[:n_dp], refs[n_dp:]
    product = jnp.dot(gather_rows(parts, slots), weight[layer], preferred_element_type=F32)
    mixed[...] = product
    sent[...] = product.astype(BF16)


def mix_last(n_dp, layer, *refs):
    parts, (weight, base, order) = refs[:n_dp], refs[n_dp : n_dp + 3]
    own, outs, slots = refs[n_dp + 3], refs[n_dp + 4 : -1], refs[-1]
    rows = own.shape[0]
    product = jnp.dot(gather_rows(parts, slots), weight[layer], preferred_element_type=F32)
    high, low = split(product)
    moved = jnp.dot(order[...], high, preferred_element_type=F32)
    first = order[:rows, :]
    own[...] = (
        moved[:rows]
        + jnp.dot(first, low, preferred_element_type=F32)
        + jnp.dot(first, base[...], preferred_element_type=F32)
    )
    for k, out in enumerate(outs):
        out[...] = moved[(k + 1) * rows : (k + 2) * rows].astype(BF16)


def close(own, *refs):
    total = own[...]
    for part in refs[:-1]:
        total = total + part[...].astype(F32)
    refs[-1][...] = total.astype(BF16)


def in_vmem(array):
    return pltpu.with_memory_space_constraint(array, pltpu.VMEM)


def stage(n_tp, n_dp, tokens, tokens_out, order_in, order_out):
    tokens_out[...] = tokens[...]
    total = order_in.shape[0]

    def held(dim, n, index):
        row = lax.broadcasted_iota(jnp.int32, (total, total), dim)
        size = total // n
        return peer_of(n, row // size, index) * size + row % size

    tp, dp = lax.axis_index("tp"), lax.axis_index("dp")
    order_in[...] = jnp.where(held(0, n_dp, dp) == held(1, n_tp, tp), 1.0, 0.0).astype(BF16)
    order_out[...] = jnp.where(held(0, n_tp, tp) == held(1, n_dp, dp), 1.0, 0.0).astype(BF16)


def call(body, args, in_specs, outs, scratch=(), flops=None):
    return pl.pallas_call(
        body,
        out_shape=[pltpu.VMEM(shape, dtype) for shape, dtype in outs],
        in_specs=in_specs,
        out_specs=[VMEM] * len(outs),
        scratch_shapes=[pltpu.VMEM(shape, dtype) for shape, dtype in scratch],
        compiler_params=pltpu.CompilerParams(vmem_limit_bytes=8 << 20),
        cost_estimate=flops and pl.CostEstimate(flops=flops, bytes_accessed=0, transcendentals=0),
    )(*map(in_vmem, args))


def per_device(
    n_tp,
    n_dp,
    tokens,
    norm_gain,
    w_query,
    w_forget,
    w_value,
    w_gate,
    lower_bound,
    head_gain,
    w_out,
    state,
):
    seqs, heads, hd = state.shape[1], state.shape[2], state.shape[3]
    rows, local = tokens.shape
    features = local * n_dp
    total = rows * n_tp
    width = heads * hd
    weights = (w_query, w_forget, w_value, w_gate)
    tokens, order_in, order_out = call(
        functools.partial(stage, n_tp, n_dp),
        (tokens,),
        [VMEM],
        [((rows, local), BF16)] + [((total, total), BF16)] * 2,
        flops=20_000_000_000,
    )
    parts = gather("tp", n_tp, tokens)
    base = mixed = None
    new_state = None
    for layer in range(2):
        outs = [((total, local), BF16), ((seqs, 4 * width + LANES), F32)]
        outs += [((seqs, 4 * width + LANES), BF16)] * (n_dp - 1)
        specs = [VMEM] * 4
        if layer == 0:
            base, own, *sent = call(
                functools.partial(project_first, n_tp, layer),
                (*parts, order_in, norm_gain, *weights),
                [VMEM] * (n_tp + 2) + specs,
                outs,
                [((total, local), F32)],
            )
        else:
            base, own, *sent = call(
                functools.partial(project_next, n_tp, layer),
                (base, mixed, *parts, norm_gain, *weights),
                [VMEM] * (n_tp + 2) + specs,
                outs,
            )
        parts = exchange("dp", n_dp, sent)
        normed, gates = call(
            functools.partial(recur, n_dp, layer, features),
            (own, *parts, lower_bound, head_gain, state),
            [VMEM] * (n_dp + 2) + [VMEM],
            [((seqs, width), BF16), ((seqs, 3, width), F32)],
        )
        parts = gather("dp", n_dp, normed)
        new_state = pl.pallas_call(
            functools.partial(update, layer),
            name="update",
            out_shape=jax.ShapeDtypeStruct(state.shape, F32),
            in_specs=[VMEM, VMEM] + ([ANY] if layer else []),
            out_specs=ANY,
            input_output_aliases={2: 0} if layer else {},
            scratch_shapes=[
                pltpu.VMEM((seqs, heads, hd, hd), F32),
                pltpu.SemaphoreType.DMA((seqs,)),
            ],
            compiler_params=pltpu.CompilerParams(vmem_limit_bytes=4 << 20),
        )(in_vmem(gates), in_vmem(state), *((new_state,) if layer else ()))
        if layer == 0:
            mixed, sent = call(
                functools.partial(mix_next, n_dp, layer),
                (*parts, w_out),
                [VMEM] * n_dp + [VMEM],
                [((total, local), F32), ((total, local), BF16)],
                [((total, width), F32)],
            )
            parts = exchange("tp", n_tp, [sent] * (n_tp - 1))
        else:
            own, *sent = call(
                functools.partial(mix_last, n_dp, layer),
                (*parts, w_out, base, order_out),
                [VMEM] * n_dp + [VMEM] + [VMEM] * 2,
                [((rows, local), F32)] + [((rows, local), BF16)] * (n_tp - 1),
                [((total, width), F32)],
            )
            parts = exchange("tp", n_tp, sent)
    hidden = pl.pallas_call(
        close,
        name="close",
        out_shape=jax.ShapeDtypeStruct((rows, local), BF16),
        in_specs=[VMEM] * n_tp,
        out_specs=VMEM,
        compiler_params=pltpu.CompilerParams(vmem_limit_bytes=4 << 20),
    )(*map(in_vmem, (own, *parts)))
    return (hidden, new_state)


def solution(mesh):
    n_tp, n_dp = mesh.shape["tp"], mesh.shape["dp"]

    def body(*args):
        return per_device(n_tp, n_dp, *args)

    return jax.shard_map(
        body,
        mesh=mesh,
        in_specs=(
            P(("grp", "tp"), "dp"),
            P(None, "dp"),
            P(None, "dp", "tp"),
            P(None, "dp", "tp"),
            P(None, "dp", "tp"),
            P(None, "dp", "tp"),
            P(None, "tp"),
            P(),
            P(None, "tp", "dp"),
            P(None, ("grp", "dp"), "tp", None, None),
        ),
        out_specs=(P(("grp", "tp"), "dp"), P(None, ("grp", "dp"), "tp", None, None)),
        check_vma=False,
    )
```

```python
import functools

import jax
import jax.numpy as jnp
from jax import lax
from jax.experimental import pallas as pl
from jax.experimental.pallas import tpu as pltpu
from jax.sharding import PartitionSpec as P


F32, BF16 = jnp.float32, jnp.bfloat16
LANES = 128
VMEM = pl.BlockSpec(memory_space=pltpu.VMEM)
ANY = pl.BlockSpec(memory_space=pl.ANY)


def peer_of(n, k, index):
    if n & (n - 1) == 0:
        return index ^ k
    return (index + k) % n


def exchange(axis, n, arrays, inward=False):
    parts = [None] * (n - 1)
    for k in reversed(range(1, n)):
        pairs = [(i, peer_of(n, k, i)) for i in range(n)]
        parts[k - 1] = lax.ppermute(
            arrays[k - 1], axis, [(b, a) for a, b in pairs] if inward else pairs
        )
    return parts


def gather(axis, n, array):
    return [array] + exchange(axis, n, [array] * (n - 1), inward=True)


def split(array):
    high = array.astype(BF16)
    return high, (array - high.astype(F32)).astype(BF16)


def finish_projection(base, gain_ref, layer, weights, outs):
    count = outs[0].shape[0]
    squares = jnp.sum(base * base, axis=1, keepdims=True)
    scaled = (base * gain_ref[layer : layer + 1, :]).astype(BF16)
    high, _ = split(squares)
    high = high.astype(F32)
    middle, low = split(squares - high)
    lane = lax.broadcasted_iota(jnp.int32, (base.shape[0], LANES), 1)
    zero = jnp.zeros((base.shape[0], LANES), F32)
    tail = jnp.where(lane == 0, high, zero)
    tail = jnp.where(lane == 1, middle.astype(F32), tail)
    tail = jnp.where(lane == 2, low.astype(F32), tail)
    width = weights[0].shape[-1]
    for index, weight in enumerate(weights):
        product = jnp.dot(scaled, weight[layer], preferred_element_type=F32)
        for k, out in enumerate(outs):
            out[:, index * width : (index + 1) * width] = product[
                k * count : (k + 1) * count
            ].astype(out.dtype)
    for k, out in enumerate(outs):
        out[:, 4 * width :] = tail[k * count : (k + 1) * count].astype(out.dtype)


def project_first(n_tp, layer, *refs):
    parts, (order, gain), weights = refs[:n_tp], refs[n_tp : n_tp + 2], refs[n_tp + 2 : n_tp + 6]
    base_out, outs, slots = refs[n_tp + 6], refs[n_tp + 7 : -1], refs[-1]
    rows = parts[0].shape[0]
    for k, part in enumerate(parts):
        slots[k * rows : (k + 1) * rows, :] = part[...].astype(F32)
    base = jnp.dot(order[...], slots[...].astype(BF16), preferred_element_type=F32)
    base_out[...] = base.astype(BF16)
    finish_projection(base, gain, layer, weights, outs)


def project_next(n_tp, layer, *refs):
    (base_in, mixed), parts = refs[:2], refs[2 : n_tp + 1]
    gain, weights = refs[n_tp + 1], refs[n_tp + 2 : n_tp + 6]
    base_out, outs = refs[n_tp + 6], refs[n_tp + 7 :]
    base = base_in[...].astype(F32) + mixed[...]
    for part in parts:
        base = base + part[...].astype(F32)
    rounded = base.astype(BF16)
    base_out[...] = rounded
    finish_projection(rounded.astype(F32), gain, layer, weights, outs)


def recur(n_dp, layer, features, *refs):
    own, parts = refs[0], refs[1:n_dp]
    bound_ref, head_gain, state, normed, gates = refs[n_dp:]
    seqs, heads, hd = state.shape[1], state.shape[2], state.shape[3]
    width = heads * hd
    total = own[...]
    for part in parts:
        total = total + part[...].astype(F32)
    mean = jnp.sum(total[:, 4 * width :], axis=1, keepdims=True) / features
    factor = lax.rsqrt(mean + 1e-06)
    query, forget_pre, value, gate_pre = (
        total[:, index * width : (index + 1) * width] * factor for index in range(4)
    )
    bound = bound_ref[layer : layer + 1, :]
    forget = bound + (1.0 - bound) * jax.nn.sigmoid(forget_pre)
    keyvec = (1.0 - bound) * jax.nn.sigmoid(-forget_pre)
    for seq in range(seqs):
        for index, vector in enumerate((forget, keyvec, value)):
            gates[seq, index : index + 1, :] = vector[seq : seq + 1]
    gate = jax.nn.sigmoid(gate_pre)
    weighted = query * forget
    shared = query * keyvec
    row = lax.broadcasted_iota(jnp.int32, (seqs, hd), 0)
    for head in range(heads):
        cols = slice(head * hd, (head + 1) * hd)
        readout = jnp.sum(shared[:, cols], axis=1, keepdims=True) * value[:, cols]
        for seq in range(seqs):
            high, low = split(jnp.where(row == seq, weighted[:, cols], 0.0))
            stored = state[layer, seq, head].astype(BF16)
            readout = readout + jnp.dot(high, stored, preferred_element_type=F32)
            readout = readout + jnp.dot(low, stored, preferred_element_type=F32)
        scale = lax.rsqrt(jnp.mean(readout * readout, axis=1, keepdims=True) + 1e-06)
        normed[:, cols] = (
            readout * scale * head_gain[layer : layer + 1, :] * gate[:, cols]
        ).astype(BF16)


def update(layer, gates, state, *refs):
    out, staged, sems = refs[-3:]
    seqs, heads, hd = state.shape[1], state.shape[2], state.shape[3]
    copies = []
    for seq in range(seqs):
        for head in range(heads):
            cols = slice(head * hd, (head + 1) * hd)
            forget, keyvec, value = (gates[seq, index : index + 1, cols] for index in range(3))
            forget = jnp.transpose(jnp.broadcast_to(forget, (hd, hd)))
            keyvec = jnp.transpose(jnp.broadcast_to(keyvec, (hd, hd)))
            staged[seq, head] = forget * state[layer, seq, head] + keyvec * value
        copies.append(pltpu.make_async_copy(staged.at[seq], out.at[layer, seq], sems.at[seq]))
        copies[-1].start()
    for copy in copies:
        copy.wait()


def gather_rows(parts, slots):
    rows = parts[0].shape[0]
    for k, part in enumerate(parts):
        slots[k * rows : (k + 1) * rows, :] = part[...].astype(F32)
    return slots[...].astype(BF16)


def mix_next(n_dp, layer, *refs):
    parts, (weight, mixed, sent, slots) = refs[:n_dp], refs[n_dp:]
    product = jnp.dot(gather_rows(parts, slots), weight[layer], preferred_element_type=F32)
    mixed[...] = product
    sent[...] = product.astype(BF16)


def mix_last(n_dp, layer, *refs):
    parts, (weight, base, order) = refs[:n_dp], refs[n_dp : n_dp + 3]
    own, outs, slots = refs[n_dp + 3], refs[n_dp + 4 : -1], refs[-1]
    rows = own.shape[0]
    product = jnp.dot(gather_rows(parts, slots), weight[layer], preferred_element_type=F32)
    high, low = split(product)
    moved = jnp.dot(order[...], high, preferred_element_type=F32)
    first = order[:rows, :]
    own[...] = (
        moved[:rows]
        + jnp.dot(first, low, preferred_element_type=F32)
        + jnp.dot(first, base[...], preferred_element_type=F32)
    )
    for k, out in enumerate(outs):
        out[...] = moved[(k + 1) * rows : (k + 2) * rows].astype(BF16)


def close(own, *refs):
    total = own[...]
    for part in refs[:-1]:
        total = total + part[...].astype(F32)
    refs[-1][...] = total.astype(BF16)


def in_vmem(array):
    return pltpu.with_memory_space_constraint(array, pltpu.VMEM)


def stage(n_tp, n_dp, order_in, order_out):
    total = order_in.shape[0]

    def held(dim, n, index):
        row = lax.broadcasted_iota(jnp.int32, (total, total), dim)
        size = total // n
        return peer_of(n, row // size, index) * size + row % size

    tp, dp = lax.axis_index("tp"), lax.axis_index("dp")
    order_in[...] = jnp.where(held(0, n_dp, dp) == held(1, n_tp, tp), 1.0, 0.0).astype(BF16)
    order_out[...] = jnp.where(held(0, n_tp, tp) == held(1, n_dp, dp), 1.0, 0.0).astype(BF16)


def call(body, args, in_specs, outs, scratch=(), flops=None):
    return pl.pallas_call(
        body,
        out_shape=[pltpu.VMEM(shape, dtype) for shape, dtype in outs],
        in_specs=in_specs,
        out_specs=[VMEM] * len(outs),
        scratch_shapes=[pltpu.VMEM(shape, dtype) for shape, dtype in scratch],
        compiler_params=pltpu.CompilerParams(vmem_limit_bytes=8 << 20),
        cost_estimate=flops and pl.CostEstimate(flops=flops, bytes_accessed=0, transcendentals=0),
    )(*map(in_vmem, args))


def per_device(
    n_tp,
    n_dp,
    tokens,
    norm_gain,
    w_query,
    w_forget,
    w_value,
    w_gate,
    lower_bound,
    head_gain,
    w_out,
    state,
):
    seqs, heads, hd = state.shape[1], state.shape[2], state.shape[3]
    rows, local = tokens.shape
    features = local * n_dp
    total = rows * n_tp
    width = heads * hd
    weights = (w_query, w_forget, w_value, w_gate)
    order_in, order_out = call(
        functools.partial(stage, n_tp, n_dp),
        (),
        [],
        [((total, total), BF16)] * 2,
        flops=20_000_000_000,
    )
    parts = gather("tp", n_tp, tokens)
    base = mixed = None
    new_state = None
    for layer in range(2):
        outs = [((total, local), BF16), ((seqs, 4 * width + LANES), F32)]
        outs += [((seqs, 4 * width + LANES), BF16)] * (n_dp - 1)
        specs = [VMEM] * 4
        if layer == 0:
            base, own, *sent = call(
                functools.partial(project_first, n_tp, layer),
                (*parts, order_in, norm_gain, *weights),
                [VMEM] * (n_tp + 2) + specs,
                outs,
                [((total, local), F32)],
            )
        else:
            base, own, *sent = call(
                functools.partial(project_next, n_tp, layer),
                (base, mixed, *parts, norm_gain, *weights),
                [VMEM] * (n_tp + 2) + specs,
                outs,
            )
        parts = exchange("dp", n_dp, sent)
        normed, gates = call(
            functools.partial(recur, n_dp, layer, features),
            (own, *parts, lower_bound, head_gain, state),
            [VMEM] * (n_dp + 2) + [VMEM],
            [((seqs, width), BF16), ((seqs, 3, width), F32)],
        )
        parts = gather("dp", n_dp, normed)
        new_state = pl.pallas_call(
            functools.partial(update, layer),
            name="update",
            out_shape=jax.ShapeDtypeStruct(state.shape, F32),
            in_specs=[VMEM, VMEM] + ([ANY] if layer else []),
            out_specs=ANY,
            input_output_aliases={2: 0} if layer else {},
            scratch_shapes=[
                pltpu.VMEM((seqs, heads, hd, hd), F32),
                pltpu.SemaphoreType.DMA((seqs,)),
            ],
            compiler_params=pltpu.CompilerParams(vmem_limit_bytes=4 << 20),
        )(in_vmem(gates), in_vmem(state), *((new_state,) if layer else ()))
        if layer == 0:
            mixed, sent = call(
                functools.partial(mix_next, n_dp, layer),
                (*parts, w_out),
                [VMEM] * n_dp + [VMEM],
                [((total, local), F32), ((total, local), BF16)],
                [((total, width), F32)],
            )
            parts = exchange("tp", n_tp, [sent] * (n_tp - 1))
        else:
            own, *sent = call(
                functools.partial(mix_last, n_dp, layer),
                (*parts, w_out, base, order_out),
                [VMEM] * n_dp + [VMEM] + [VMEM] * 2,
                [((rows, local), F32)] + [((rows, local), BF16)] * (n_tp - 1),
                [((total, width), F32)],
            )
            parts = exchange("tp", n_tp, sent)
    hidden = pl.pallas_call(
        close,
        name="close",
        out_shape=jax.ShapeDtypeStruct((rows, local), BF16),
        in_specs=[VMEM] * n_tp,
        out_specs=VMEM,
        compiler_params=pltpu.CompilerParams(vmem_limit_bytes=4 << 20),
    )(*map(in_vmem, (own, *parts)))
    return (hidden, new_state)


def solution(mesh):
    n_tp, n_dp = mesh.shape["tp"], mesh.shape["dp"]

    def body(*args):
        return per_device(n_tp, n_dp, *args)

    return jax.shard_map(
        body,
        mesh=mesh,
        in_specs=(
            P(("grp", "tp"), "dp"),
            P(None, "dp"),
            P(None, "dp", "tp"),
            P(None, "dp", "tp"),
            P(None, "dp", "tp"),
            P(None, "dp", "tp"),
            P(None, "tp"),
            P(),
            P(None, "tp", "dp"),
            P(None, ("grp", "dp"), "tp", None, None),
        ),
        out_specs=(P(("grp", "tp"), "dp"), P(None, ("grp", "dp"), "tp", None, None)),
        check_vma=False,
    )
```

```python
import functools

import jax
import jax.numpy as jnp
from jax import lax
from jax.experimental import pallas as pl
from jax.experimental.pallas import tpu as pltpu
from jax.sharding import PartitionSpec as P


F32, BF16 = jnp.float32, jnp.bfloat16
LANES = 128
VMEM = pl.BlockSpec(memory_space=pltpu.VMEM)
ANY = pl.BlockSpec(memory_space=pl.ANY)


def peer_of(n, k, index):
    if n & (n - 1) == 0:
        return index ^ k
    return (index + k) % n


def exchange(axis, n, arrays, inward=False):
    parts = [None] * (n - 1)
    for k in reversed(range(1, n)):
        pairs = [(i, peer_of(n, k, i)) for i in range(n)]
        parts[k - 1] = lax.ppermute(
            arrays[k - 1], axis, [(b, a) for a, b in pairs] if inward else pairs
        )
    return parts


def core_flip(n_dp):
    return int(n_dp > 1 and n_dp & (n_dp - 1) == 0)


def cross_pairs(n_tp, n_dp, k):
    flip = core_flip(n_dp)
    return [
        (t * n_dp + d, peer_of(n_tp, k, t) * n_dp + (d ^ flip))
        for t in range(n_tp)
        for d in range(n_dp)
    ]


def cross_exchange(n_tp, n_dp, arrays):
    parts = [None] * (n_tp - 1)
    for k in reversed(range(1, n_tp)):
        parts[k - 1] = lax.ppermute(
            arrays[k - 1], ("tp", "dp"), cross_pairs(n_tp, n_dp, k)
        )
    return parts


def cross_weight(n_dp, array):
    if not core_flip(n_dp):
        return array
    return lax.ppermute(array, "dp", [(d, d ^ 1) for d in range(n_dp)])


def gather(axis, n, array):
    return [array] + exchange(axis, n, [array] * (n - 1), inward=True)


def split(array):
    high = array.astype(BF16)
    return high, (array - high.astype(F32)).astype(BF16)


def finish_projection(base, gain_ref, layer, weights, outs):
    count = outs[0].shape[0]
    squares = jnp.sum(base * base, axis=1, keepdims=True)
    scaled = (base * gain_ref[layer : layer + 1, :]).astype(BF16)
    high, _ = split(squares)
    high = high.astype(F32)
    middle, low = split(squares - high)
    lane = lax.broadcasted_iota(jnp.int32, (base.shape[0], LANES), 1)
    zero = jnp.zeros((base.shape[0], LANES), F32)
    tail = jnp.where(lane == 0, high, zero)
    tail = jnp.where(lane == 1, middle.astype(F32), tail)
    tail = jnp.where(lane == 2, low.astype(F32), tail)
    width = weights[0].shape[-1]
    for index, weight in enumerate(weights):
        product = jnp.dot(scaled, weight[layer], preferred_element_type=F32)
        for k, out in enumerate(outs):
            out[:, index * width : (index + 1) * width] = product[
                k * count : (k + 1) * count
            ].astype(out.dtype)
    for k, out in enumerate(outs):
        out[:, 4 * width :] = tail[k * count : (k + 1) * count].astype(out.dtype)


def project_first(n_tp, layer, *refs):
    parts, (order, gain), weights = refs[:n_tp], refs[n_tp : n_tp + 2], refs[n_tp + 2 : n_tp + 6]
    base_out, outs, slots = refs[n_tp + 6], refs[n_tp + 7 : -1], refs[-1]
    rows = parts[0].shape[0]
    for k, part in enumerate(parts):
        slots[k * rows : (k + 1) * rows, :] = part[...].astype(F32)
    base = jnp.dot(order[...], slots[...].astype(BF16), preferred_element_type=F32)
    base_out[...] = base.astype(BF16)
    finish_projection(base, gain, layer, weights, outs)


def project_next(n_tp, layer, *refs):
    (base_in, mixed), parts = refs[:2], refs[2 : n_tp + 1]
    gain, weights = refs[n_tp + 1], refs[n_tp + 2 : n_tp + 6]
    base_out, outs = refs[n_tp + 6], refs[n_tp + 7 :]
    base = base_in[...].astype(F32) + mixed[...]
    for part in parts:
        base = base + part[...].astype(F32)
    rounded = base.astype(BF16)
    base_out[...] = rounded
    finish_projection(rounded.astype(F32), gain, layer, weights, outs)


def recur(n_dp, layer, features, *refs):
    own, parts = refs[0], refs[1:n_dp]
    bound_ref, head_gain, state, normed, gates, left = refs[n_dp:]
    seqs, heads, hd = state.shape[1], state.shape[2], state.shape[3]
    width = heads * hd
    total = own[...]
    for part in parts:
        total = total + part[...].astype(F32)
    mean = jnp.sum(total[:, 4 * width :], axis=1, keepdims=True) / features
    factor = lax.rsqrt(mean + 1e-06)
    query, forget_pre, value, gate_pre = (
        total[:, index * width : (index + 1) * width] * factor for index in range(4)
    )
    bound = bound_ref[layer : layer + 1, :]
    forget = bound + (1.0 - bound) * jax.nn.sigmoid(forget_pre)
    keyvec = (1.0 - bound) * jax.nn.sigmoid(-forget_pre)
    for seq in range(seqs):
        for index, vector in enumerate((forget, keyvec, value)):
            gates[seq, index : index + 1, :] = vector[seq : seq + 1]
    gate = jax.nn.sigmoid(gate_pre)
    weighted = query * forget
    shared = query * keyvec
    row = lax.broadcasted_iota(jnp.int32, (seqs, hd), 0)
    terms = [term.astype(F32) for term in split(weighted)]
    group = 2 if heads % 2 == 0 else 1
    for first in range(0, heads, group):
        for index in range(group):
            cols = slice((first + index) * hd, (first + index + 1) * hd)
            for part, term in enumerate(terms):
                top = (index * 2 + part) * seqs
                for seq in range(seqs):
                    left[top : top + seqs, seq * hd : (seq + 1) * hd] = jnp.where(
                        row == seq, term[:, cols], 0.0
                    )
        right = jnp.concatenate(
            [
                jnp.concatenate(
                    [state[layer, seq, first + index].astype(BF16) for seq in range(seqs)], axis=0
                )
                for index in range(group)
            ],
            axis=1,
        )
        product = jnp.dot(
            left[: 2 * group * seqs, :].astype(BF16), right, preferred_element_type=F32
        )
        for index in range(group):
            head = first + index
            cols = slice(head * hd, (head + 1) * hd)
            own_cols = slice(index * hd, (index + 1) * hd)
            readout = jnp.sum(shared[:, cols], axis=1, keepdims=True) * value[:, cols]
            for part in range(2):
                top = (index * 2 + part) * seqs
                readout = readout + product[top : top + seqs, own_cols]
            scale = lax.rsqrt(jnp.mean(readout * readout, axis=1, keepdims=True) + 1e-06)
            normed[:, cols] = (
                readout * scale * head_gain[layer : layer + 1, :] * gate[:, cols]
            ).astype(BF16)


def update(layer, gates, state, *refs):
    out, staged, sems = refs[-3:]
    seqs, heads, hd = state.shape[1], state.shape[2], state.shape[3]
    copies = []
    for seq in range(seqs):
        for head in range(heads):
            cols = slice(head * hd, (head + 1) * hd)
            forget, keyvec, value = (gates[seq, index : index + 1, cols] for index in range(3))
            forget = jnp.transpose(jnp.broadcast_to(forget, (hd, hd)))
            keyvec = jnp.transpose(jnp.broadcast_to(keyvec, (hd, hd)))
            staged[seq, head] = forget * state[layer, seq, head] + keyvec * value
        copies.append(pltpu.make_async_copy(staged.at[seq], out.at[layer, seq], sems.at[seq]))
        copies[-1].start()
    for copy in copies:
        copy.wait()


def gather_rows(parts, slots):
    rows = parts[0].shape[0]
    for k, part in enumerate(parts):
        slots[k * rows : (k + 1) * rows, :] = part[...].astype(F32)
    return slots[...].astype(BF16)


def mix_next(n_dp, layer, *refs):
    parts, (weight, crossed, mixed, sent, slots) = refs[:n_dp], refs[n_dp:]
    facing = [parts[k ^ core_flip(n_dp)] for k in range(n_dp)]
    rows = gather_rows(facing, slots)
    sent[...] = jnp.dot(rows, crossed[layer], preferred_element_type=F32).astype(BF16)
    rows = gather_rows(parts, slots)
    mixed[...] = jnp.dot(rows, weight[layer], preferred_element_type=F32)


def mix_last(n_dp, layer, *refs):
    parts, (weight, crossed, base, order) = refs[:n_dp], refs[n_dp : n_dp + 4]
    own, outs, slots = refs[n_dp + 4], refs[n_dp + 5 : -1], refs[-1]
    rows = own.shape[0]
    moved = jnp.dot(order[...], gather_rows(parts, slots), preferred_element_type=F32)
    moved = moved.astype(BF16)
    product = jnp.dot(moved, crossed[layer], preferred_element_type=F32)
    for k, out in enumerate(outs):
        out[...] = product[(k + 1) * rows : (k + 2) * rows].astype(BF16)
    own[...] = jnp.dot(moved, weight[layer], preferred_element_type=F32)[:rows] + jnp.dot(
        order[:rows, :], base[...], preferred_element_type=F32
    )


def close(own, *refs):
    total = own[...]
    for part in refs[:-1]:
        total = total + part[...].astype(F32)
    refs[-1][...] = total.astype(BF16)


def in_vmem(array):
    return pltpu.with_memory_space_constraint(array, pltpu.VMEM)


def stage(n_tp, n_dp, order_in, order_out):
    total = order_in.shape[0]

    def held(dim, n, index):
        row = lax.broadcasted_iota(jnp.int32, (total, total), dim)
        size = total // n
        return peer_of(n, row // size, index) * size + row % size

    tp, dp = lax.axis_index("tp"), lax.axis_index("dp")
    order_in[...] = jnp.where(held(0, n_dp, dp) == held(1, n_tp, tp), 1.0, 0.0).astype(BF16)
    order_out[...] = jnp.where(held(0, n_tp, tp) == held(1, n_dp, dp), 1.0, 0.0).astype(BF16)


def call(body, args, in_specs, outs, scratch=(), flops=None):
    return pl.pallas_call(
        body,
        out_shape=[pltpu.VMEM(shape, dtype) for shape, dtype in outs],
        in_specs=in_specs,
        out_specs=[VMEM] * len(outs),
        scratch_shapes=[pltpu.VMEM(shape, dtype) for shape, dtype in scratch],
        compiler_params=pltpu.CompilerParams(vmem_limit_bytes=8 << 20),
        cost_estimate=flops and pl.CostEstimate(flops=flops, bytes_accessed=0, transcendentals=0),
    )(*map(in_vmem, args))


def per_device(
    n_tp,
    n_dp,
    tokens,
    norm_gain,
    w_query,
    w_forget,
    w_value,
    w_gate,
    lower_bound,
    head_gain,
    w_out,
    state,
):
    seqs, heads, hd = state.shape[1], state.shape[2], state.shape[3]
    rows, local = tokens.shape
    features = local * n_dp
    total = rows * n_tp
    width = heads * hd
    weights = (w_query, w_forget, w_value, w_gate)
    order_in, order_out = call(
        functools.partial(stage, n_tp, n_dp),
        (),
        [],
        [((total, total), BF16)] * 2,
        flops=20_000_000_000,
    )
    parts = gather("tp", n_tp, tokens)
    crossed = cross_weight(n_dp, w_out)
    base = mixed = None
    new_state = None
    for layer in range(2):
        outs = [((total, local), BF16), ((seqs, 4 * width + LANES), F32)]
        outs += [((seqs, 4 * width + LANES), BF16)] * (n_dp - 1)
        specs = [VMEM] * 4
        if layer == 0:
            base, own, *sent = call(
                functools.partial(project_first, n_tp, layer),
                (*parts, order_in, norm_gain, *weights),
                [VMEM] * (n_tp + 2) + specs,
                outs,
                [((total, local), F32)],
            )
        else:
            base, own, *sent = call(
                functools.partial(project_next, n_tp, layer),
                (base, mixed, *parts, norm_gain, *weights),
                [VMEM] * (n_tp + 2) + specs,
                outs,
            )
        parts = exchange("dp", n_dp, sent)
        normed, gates = call(
            functools.partial(recur, n_dp, layer, features),
            (own, *parts, lower_bound, head_gain, state),
            [VMEM] * (n_dp + 2) + [VMEM],
            [((seqs, width), BF16), ((seqs, 3, width), F32)],
            [((4 * seqs, seqs * hd), F32)],
        )
        parts = gather("dp", n_dp, normed)
        new_state = pl.pallas_call(
            functools.partial(update, layer),
            name="update",
            out_shape=jax.ShapeDtypeStruct(state.shape, F32),
            in_specs=[VMEM, VMEM] + ([ANY] if layer else []),
            out_specs=ANY,
            input_output_aliases={2: 0} if layer else {},
            scratch_shapes=[
                pltpu.VMEM((seqs, heads, hd, hd), F32),
                pltpu.SemaphoreType.DMA((seqs,)),
            ],
            compiler_params=pltpu.CompilerParams(vmem_limit_bytes=4 << 20),
        )(in_vmem(gates), in_vmem(state), *((new_state,) if layer else ()))
        if layer == 0:
            mixed, sent = call(
                functools.partial(mix_next, n_dp, layer),
                (*parts, w_out, crossed),
                [VMEM] * (n_dp + 2),
                [((total, local), F32), ((total, local), BF16)],
                [((total, width), F32)],
            )
            parts = cross_exchange(n_tp, n_dp, [sent] * (n_tp - 1))
        else:
            own, *sent = call(
                functools.partial(mix_last, n_dp, layer),
                (*parts, w_out, crossed, base, order_out),
                [VMEM] * (n_dp + 4),
                [((rows, local), F32)] + [((rows, local), BF16)] * (n_tp - 1),
                [((total, width), F32)],
            )
            parts = cross_exchange(n_tp, n_dp, sent)
    hidden = pl.pallas_call(
        close,
        name="close",
        out_shape=jax.ShapeDtypeStruct((rows, local), BF16),
        in_specs=[VMEM] * n_tp,
        out_specs=VMEM,
        compiler_params=pltpu.CompilerParams(vmem_limit_bytes=4 << 20),
    )(*map(in_vmem, (own, *parts)))
    return (hidden, new_state)


def solution(mesh):
    n_tp, n_dp = mesh.shape["tp"], mesh.shape["dp"]

    def body(*args):
        return per_device(n_tp, n_dp, *args)

    return jax.shard_map(
        body,
        mesh=mesh,
        in_specs=(
            P(("grp", "tp"), "dp"),
            P(None, "dp"),
            P(None, "dp", "tp"),
            P(None, "dp", "tp"),
            P(None, "dp", "tp"),
            P(None, "dp", "tp"),
            P(None, "tp"),
            P(),
            P(None, "tp", "dp"),
            P(None, ("grp", "dp"), "tp", None, None),
        ),
        out_specs=(P(("grp", "tp"), "dp"), P(None, ("grp", "dp"), "tp", None, None)),
        check_vma=False,
    )
```

```python
import functools

import jax
import jax.numpy as jnp
from jax import lax
from jax.experimental import pallas as pl
from jax.experimental.pallas import tpu as pltpu
from jax.sharding import PartitionSpec as P


F32, BF16 = jnp.float32, jnp.bfloat16
LANES = 128
VMEM = pl.BlockSpec(memory_space=pltpu.VMEM)
ANY = pl.BlockSpec(memory_space=pl.ANY)


def peer_of(n, k, index):
    if n & (n - 1) == 0:
        return index ^ k
    return (index + k) % n


def chip_rounds(n_dp):
    return list(range(3, n_dp, 2)) if core_flip(n_dp) else list(range(1, n_dp))


def exchange(axis, n, arrays, inward=False, rounds=None):
    rounds = rounds or list(range(1, n))
    parts = {}
    for k, array in reversed(list(zip(rounds, arrays))):
        pairs = [(i, peer_of(n, k, i)) for i in range(n)]
        parts[k] = lax.ppermute(array, axis, [(b, a) for a, b in pairs] if inward else pairs)
    return [parts[k] for k in rounds]


def core_flip(n_dp):
    return int(n_dp > 1 and n_dp & (n_dp - 1) == 0)


def cross_pairs(n_tp, n_dp, k):
    flip = core_flip(n_dp)
    return [
        (t * n_dp + d, peer_of(n_tp, k, t) * n_dp + (d ^ flip))
        for t in range(n_tp)
        for d in range(n_dp)
    ]


def cross_exchange(n_tp, n_dp, arrays):
    parts = [None] * (n_tp - 1)
    for k in reversed(range(1, n_tp)):
        parts[k - 1] = lax.ppermute(
            arrays[k - 1], ("tp", "dp"), cross_pairs(n_tp, n_dp, k)
        )
    return parts


def cross_copy(n_dp, array):
    if not core_flip(n_dp):
        return array
    return lax.ppermute(array, "dp", [(d, d ^ 1) for d in range(n_dp)])


def gather(axis, n, array, rounds=None):
    rounds = list(range(1, n)) if rounds is None else rounds
    if not rounds:
        return [array]
    return [array] + exchange(axis, n, [array] * len(rounds), True, rounds)


def split(array):
    high = array.astype(BF16)
    return high, (array - high.astype(F32)).astype(BF16)


def finish_projection(base, gain_ref, layer, weights, outs):
    count = base.shape[0] // len(outs)
    group = outs[0].shape[0] // count
    squares = jnp.sum(base * base, axis=1, keepdims=True)
    scaled = (base * gain_ref[layer : layer + 1, :]).astype(BF16)
    high, _ = split(squares)
    high = high.astype(F32)
    middle, low = split(squares - high)
    lane = lax.broadcasted_iota(jnp.int32, (base.shape[0], LANES), 1)
    zero = jnp.zeros((base.shape[0], LANES), F32)
    tail = jnp.where(lane == 0, high, zero)
    tail = jnp.where(lane == 1, middle.astype(F32), tail)
    tail = jnp.where(lane == 2, low.astype(F32), tail)
    width = weights[0].shape[-1]
    for index, weight in enumerate(weights):
        product = jnp.dot(scaled, weight[layer], preferred_element_type=F32)
        for k, out in enumerate(outs):
            for member in range(group):
                block = slice((k ^ member) * count, ((k ^ member) + 1) * count)
                rows = slice(member * count, (member + 1) * count)
                out[rows, index * width : (index + 1) * width] = product[block].astype(out.dtype)
    for k, out in enumerate(outs):
        for member in range(group):
            block = slice((k ^ member) * count, ((k ^ member) + 1) * count)
            rows = slice(member * count, (member + 1) * count)
            out[rows, 4 * width :] = tail[block].astype(out.dtype)


def project_first(n_tp, layer, *refs):
    parts, (order, gain), weights = refs[:n_tp], refs[n_tp : n_tp + 2], refs[n_tp + 2 : n_tp + 6]
    base_out, outs, slots = refs[n_tp + 6], refs[n_tp + 7 : -1], refs[-1]
    rows = parts[0].shape[0]
    for k, part in enumerate(parts):
        slots[k * rows : (k + 1) * rows, :] = part[...].astype(F32)
    base = jnp.dot(order[...], slots[...].astype(BF16), preferred_element_type=F32)
    base_out[...] = base.astype(BF16)
    finish_projection(base, gain, layer, weights, outs)


def project_next(n_tp, layer, *refs):
    held, parts = refs[0], refs[1:n_tp]
    gain, weights = refs[n_tp], refs[n_tp + 1 : n_tp + 5]
    base_out, outs = refs[n_tp + 5], refs[n_tp + 6 :]
    base = held[...]
    for part in parts:
        base = base + part[...].astype(F32)
    rounded = base.astype(BF16)
    base_out[...] = rounded
    finish_projection(rounded.astype(F32), gain, layer, weights, outs)


def recur(n_dp, layer, features, group, *refs):
    own, parts = refs[0], refs[1:n_dp]
    (bound_ref, head_gain), states = refs[n_dp : n_dp + 2], refs[n_dp + 2 : n_dp + 2 + group]
    normed, gates, left = refs[n_dp + 2 + group :]
    kept, heads, hd = states[0].shape[1:4]
    seqs = group * kept
    width = heads * hd
    total = own[...]
    for part in parts:
        total = total + part[...].astype(F32)
    mean = jnp.sum(total[:, 4 * width :], axis=1, keepdims=True) / features
    factor = lax.rsqrt(mean + 1e-06)
    query, forget_pre, value, gate_pre = (
        total[:, index * width : (index + 1) * width] * factor for index in range(4)
    )
    bound = bound_ref[layer : layer + 1, :]
    forget = bound + (1.0 - bound) * jax.nn.sigmoid(forget_pre)
    keyvec = (1.0 - bound) * jax.nn.sigmoid(-forget_pre)
    for seq in range(kept):
        for index, vector in enumerate((forget, keyvec, value)):
            gates[seq, index : index + 1, :] = vector[seq : seq + 1]
    gate = jax.nn.sigmoid(gate_pre)
    weighted = query * forget
    shared = query * keyvec
    row = lax.broadcasted_iota(jnp.int32, (seqs, hd), 0)
    terms = [term.astype(F32) for term in split(weighted)]
    wide = 2 if heads % 2 == 0 else 1
    for first in range(0, heads, wide):
        for index in range(wide):
            cols = slice((first + index) * hd, (first + index + 1) * hd)
            for part, term in enumerate(terms):
                top = (index * 2 + part) * seqs
                for seq in range(seqs):
                    left[top : top + seqs, seq * hd : (seq + 1) * hd] = jnp.where(
                        row == seq, term[:, cols], 0.0
                    )
        right = jnp.concatenate(
            [
                jnp.concatenate(
                    [
                        states[seq // kept][layer, seq % kept, first + index]
                        for seq in range(seqs)
                    ],
                    axis=0,
                )
                for index in range(wide)
            ],
            axis=1,
        )
        product = jnp.dot(
            left[: 2 * wide * seqs, :].astype(BF16), right, preferred_element_type=F32
        )
        for index in range(wide):
            head = first + index
            cols = slice(head * hd, (head + 1) * hd)
            own_cols = slice(index * hd, (index + 1) * hd)
            readout = jnp.sum(shared[:, cols], axis=1, keepdims=True) * value[:, cols]
            for part in range(2):
                top = (index * 2 + part) * seqs
                readout = readout + product[top : top + seqs, own_cols]
            scale = lax.rsqrt(jnp.mean(readout * readout, axis=1, keepdims=True) + 1e-06)
            normed[:, cols] = (
                readout * scale * head_gain[layer : layer + 1, :] * gate[:, cols]
            ).astype(BF16)


def update(layer, gates, state, *refs):
    out, staged, sems = refs[-3:]
    seqs, heads, hd = state.shape[1], state.shape[2], state.shape[3]
    copies = []
    for seq in range(seqs):
        for head in range(heads):
            cols = slice(head * hd, (head + 1) * hd)
            forget, keyvec, value = (gates[seq, index : index + 1, cols] for index in range(3))
            forget = jnp.transpose(jnp.broadcast_to(forget, (hd, hd)))
            keyvec = jnp.transpose(jnp.broadcast_to(keyvec, (hd, hd)))
            staged[seq, head] = forget * state[layer, seq, head] + keyvec * value
        copies.append(pltpu.make_async_copy(staged.at[seq], out.at[layer, seq], sems.at[seq]))
        copies[-1].start()
    for copy in copies:
        copy.wait()


def narrow(state, out, staged, sems):
    places = [(layer, seq) for layer in range(state.shape[0]) for seq in range(state.shape[1])]
    copies = [
        pltpu.make_async_copy(state.at[place], staged.at[place], sems.at[index])
        for index, place in enumerate(places)
    ]
    for copy in copies:
        copy.start()
    for copy, place in zip(copies, places):
        copy.wait()
        out[place] = staged[place].astype(BF16)


def slot_parts(refs, group):
    count = refs[0].shape[0] // group
    if group == 1:
        return [(ref, 0, count) for ref in refs]
    parts = [(refs[0], 0, count), (refs[0], count, count)]
    for ref in refs[1:]:
        parts += [(ref, count, count), (ref, 0, count)]
    return parts


def gather_rows(parts, slots):
    for k, (ref, top, count) in enumerate(parts):
        slots[k * count : (k + 1) * count, :] = ref[top : top + count, :].astype(F32)
    return slots[...].astype(BF16)


def mix_next(n_chip, group, layer, *refs):
    parts, (crossed, sent, slots) = slot_parts(refs[:n_chip], group), refs[n_chip:]
    facing = [parts[k ^ (group - 1)] for k in range(len(parts))]
    rows = gather_rows(facing, slots)
    sent[...] = jnp.dot(rows, crossed[layer], preferred_element_type=F32).astype(BF16)


def own_next(n_chip, group, layer, *refs):
    parts, (weight, base, held, slots) = slot_parts(refs[:n_chip], group), refs[n_chip:]
    rows = gather_rows(parts, slots)
    held[...] = base[...].astype(F32) + jnp.dot(rows, weight[layer], preferred_element_type=F32)


def mix_last(n_chip, group, layer, *refs):
    parts, (crossed, order) = slot_parts(refs[:n_chip], group), refs[n_chip : n_chip + 2]
    outs, slots = refs[n_chip + 2 : -1], refs[-1]
    rows = outs[0].shape[0]
    moved = jnp.dot(order[...], gather_rows(parts, slots), preferred_element_type=F32)
    product = jnp.dot(moved.astype(BF16), crossed[layer], preferred_element_type=F32)
    for k, out in enumerate(outs):
        out[...] = product[(k + 1) * rows : (k + 2) * rows].astype(BF16)


def own_last(n_chip, group, layer, *refs):
    parts, (weight, base, order, own, slots) = slot_parts(refs[:n_chip], group), refs[n_chip:]
    rows = own.shape[0]
    moved = jnp.dot(order[...], gather_rows(parts, slots), preferred_element_type=F32)
    own[...] = jnp.dot(moved.astype(BF16), weight[layer], preferred_element_type=F32)[
        :rows
    ] + jnp.dot(order[:rows, :], base[...], preferred_element_type=F32)


def close(own, *refs):
    total = own[...]
    for part in refs[:-1]:
        total = total + part[...].astype(F32)
    refs[-1][...] = total.astype(BF16)


def in_vmem(array):
    return pltpu.with_memory_space_constraint(array, pltpu.VMEM)


def stage(n_tp, n_dp, order_in, order_out):
    total = order_in.shape[0]

    def held(dim, n, index):
        row = lax.broadcasted_iota(jnp.int32, (total, total), dim)
        size = total // n
        return peer_of(n, row // size, index) * size + row % size

    tp, dp = lax.axis_index("tp"), lax.axis_index("dp")
    order_in[...] = jnp.where(held(0, n_dp, dp) == held(1, n_tp, tp), 1.0, 0.0).astype(BF16)
    order_out[...] = jnp.where(held(0, n_tp, tp) == held(1, n_dp, dp), 1.0, 0.0).astype(BF16)


def call(body, args, in_specs, outs, scratch=(), flops=None):
    return pl.pallas_call(
        body,
        out_shape=[pltpu.VMEM(shape, dtype) for shape, dtype in outs],
        in_specs=in_specs,
        out_specs=[VMEM] * len(outs),
        scratch_shapes=[pltpu.VMEM(shape, dtype) for shape, dtype in scratch],
        compiler_params=pltpu.CompilerParams(vmem_limit_bytes=8 << 20),
        cost_estimate=flops and pl.CostEstimate(flops=flops, bytes_accessed=0, transcendentals=0),
    )(*map(in_vmem, args))


def per_device(
    n_tp,
    n_dp,
    tokens,
    norm_gain,
    w_query,
    w_forget,
    w_value,
    w_gate,
    lower_bound,
    head_gain,
    w_out,
    state,
):
    seqs, heads, hd = state.shape[1], state.shape[2], state.shape[3]
    rows, local = tokens.shape
    features = local * n_dp
    total = rows * n_tp
    width = heads * hd
    weights = (w_query, w_forget, w_value, w_gate)
    order_in, order_out = call(
        functools.partial(stage, n_tp, n_dp),
        (),
        [],
        [((total, total), BF16)] * 2,
        flops=20_000_000_000,
    )
    parts = gather("tp", n_tp, tokens)
    flip = core_flip(n_dp)
    group, n_chip = flip + 1, n_dp // (flip + 1)
    narrowed = pl.pallas_call(
        narrow,
        name="narrow",
        out_shape=pltpu.VMEM(state.shape, BF16),
        in_specs=[ANY],
        out_specs=VMEM,
        scratch_shapes=[
            pltpu.VMEM(state.shape, F32),
            pltpu.SemaphoreType.DMA((state.shape[0] * seqs,)),
        ],
        compiler_params=pltpu.CompilerParams(vmem_limit_bytes=4 << 20),
    )(pltpu.with_memory_space_constraint(state, pltpu.HBM))
    states = [narrowed] + [cross_copy(n_dp, narrowed)] * flip
    crossed = cross_copy(n_dp, w_out)
    base = held = None
    new_state = None
    for layer in range(2):
        message = (group * seqs, 4 * width + LANES)
        outs = [((total, local), BF16), (message, F32)] + [(message, BF16)] * (n_dp - 1)
        specs = [VMEM] * 4
        if layer == 0:
            base, own, *sent = call(
                functools.partial(project_first, n_tp, layer),
                (*parts, order_in, norm_gain, *weights),
                [VMEM] * (n_tp + 2) + specs,
                outs,
                [((total, local), F32)],
            )
        else:
            base, own, *sent = call(
                functools.partial(project_next, n_tp, layer),
                (held, *parts, norm_gain, *weights),
                [VMEM] * (n_tp + 1) + specs,
                outs,
            )
        parts = exchange("dp", n_dp, sent)
        normed, gates = call(
            functools.partial(recur, n_dp, layer, features, group),
            (own, *parts, lower_bound, head_gain, *states),
            [VMEM] * (n_dp + 2 + group),
            [((group * seqs, width), BF16), ((seqs, 3, width), F32)],
            [((4 * group * seqs, group * seqs * hd), F32)],
        )
        read = gather("dp", n_dp, normed, chip_rounds(n_dp))
        slots = [((total, width), F32)]
        new_state = pl.pallas_call(
            functools.partial(update, layer),
            name="update",
            out_shape=jax.ShapeDtypeStruct(state.shape, F32),
            in_specs=[VMEM, VMEM] + ([ANY] if layer else []),
            out_specs=ANY,
            input_output_aliases={2: 0} if layer else {},
            scratch_shapes=[
                pltpu.VMEM((seqs, heads, hd, hd), F32),
                pltpu.SemaphoreType.DMA((seqs,)),
            ],
            compiler_params=pltpu.CompilerParams(vmem_limit_bytes=4 << 20),
        )(in_vmem(gates), in_vmem(state), *((new_state,) if layer else ()))
        if layer == 0:
            (sent,) = call(
                functools.partial(mix_next, n_chip, group, layer),
                (*read, crossed),
                [VMEM] * (n_chip + 1),
                [((total, local), BF16)],
                slots,
            )
            parts = cross_exchange(n_tp, n_dp, [sent] * (n_tp - 1))
            (held,) = call(
                functools.partial(own_next, n_chip, group, layer),
                (*read, w_out, base),
                [VMEM] * (n_chip + 2),
                [((total, local), F32)],
                slots,
            )
        else:
            sent = call(
                functools.partial(mix_last, n_chip, group, layer),
                (*read, crossed, order_out),
                [VMEM] * (n_chip + 2),
                [((rows, local), BF16)] * (n_tp - 1),
                slots,
            )
            parts = cross_exchange(n_tp, n_dp, sent)
            (own,) = call(
                functools.partial(own_last, n_chip, group, layer),
                (*read, w_out, base, order_out),
                [VMEM] * (n_chip + 3),
                [((rows, local), F32)],
                slots,
            )
    hidden = pl.pallas_call(
        close,
        name="close",
        out_shape=jax.ShapeDtypeStruct((rows, local), BF16),
        in_specs=[VMEM] * n_tp,
        out_specs=VMEM,
        compiler_params=pltpu.CompilerParams(vmem_limit_bytes=4 << 20),
    )(*map(in_vmem, (own, *parts)))
    return (hidden, new_state)


def solution(mesh):
    n_tp, n_dp = mesh.shape["tp"], mesh.shape["dp"]

    def body(*args):
        return per_device(n_tp, n_dp, *args)

    return jax.shard_map(
        body,
        mesh=mesh,
        in_specs=(
            P(("grp", "tp"), "dp"),
            P(None, "dp"),
            P(None, "dp", "tp"),
            P(None, "dp", "tp"),
            P(None, "dp", "tp"),
            P(None, "dp", "tp"),
            P(None, "tp"),
            P(),
            P(None, "tp", "dp"),
            P(None, ("grp", "dp"), "tp", None, None),
        ),
        out_specs=(P(("grp", "tp"), "dp"), P(None, ("grp", "dp"), "tp", None, None)),
        check_vma=False,
    )
```

```python
import functools

import jax
import jax.numpy as jnp
from jax import lax
from jax.experimental import pallas as pl
from jax.experimental.pallas import tpu as pltpu
from jax.sharding import PartitionSpec as P


F32, BF16 = jnp.float32, jnp.bfloat16
LANES = 128
VMEM = pl.BlockSpec(memory_space=pltpu.VMEM)
ANY = pl.BlockSpec(memory_space=pl.ANY)


def peer_of(n, k, index):
    if n & (n - 1) == 0:
        return index ^ k
    return (index + k) % n


def chip_rounds(n_dp):
    return list(range(3, n_dp, 2)) if core_flip(n_dp) else list(range(1, n_dp))


def exchange(axis, n, arrays, inward=False, rounds=None):
    rounds = rounds or list(range(1, n))
    parts = {}
    for k, array in reversed(list(zip(rounds, arrays))):
        pairs = [(i, peer_of(n, k, i)) for i in range(n)]
        parts[k] = lax.ppermute(array, axis, [(b, a) for a, b in pairs] if inward else pairs)
    return [parts[k] for k in rounds]


def core_flip(n_dp):
    return int(n_dp > 1 and n_dp & (n_dp - 1) == 0)


def cross_pairs(n_tp, n_dp, k):
    flip = core_flip(n_dp)
    return [
        (t * n_dp + d, peer_of(n_tp, k, t) * n_dp + (d ^ flip))
        for t in range(n_tp)
        for d in range(n_dp)
    ]


def cross_exchange(n_tp, n_dp, arrays):
    parts = [None] * (n_tp - 1)
    for k in reversed(range(1, n_tp)):
        parts[k - 1] = lax.ppermute(
            arrays[k - 1], ("tp", "dp"), cross_pairs(n_tp, n_dp, k)
        )
    return parts


def cross_copy(n_dp, array):
    if not core_flip(n_dp):
        return array
    return lax.ppermute(array, "dp", [(d, d ^ 1) for d in range(n_dp)])


def gather(axis, n, array, rounds=None):
    rounds = list(range(1, n)) if rounds is None else rounds
    if not rounds:
        return [array]
    return [array] + exchange(axis, n, [array] * len(rounds), True, rounds)


def split(array):
    high = array.astype(BF16)
    return high, (array - high.astype(F32)).astype(BF16)


def finish_projection(base, gain_ref, layer, weights, outs):
    count = base.shape[0] // len(outs)
    group = outs[0].shape[0] // count
    squares = jnp.sum(base * base, axis=1, keepdims=True)
    scaled = (base * gain_ref[layer : layer + 1, :]).astype(BF16)
    high, _ = split(squares)
    high = high.astype(F32)
    middle, low = split(squares - high)
    lane = lax.broadcasted_iota(jnp.int32, (base.shape[0], LANES), 1)
    zero = jnp.zeros((base.shape[0], LANES), F32)
    tail = jnp.where(lane == 0, high, zero)
    tail = jnp.where(lane == 1, middle.astype(F32), tail)
    tail = jnp.where(lane == 2, low.astype(F32), tail)
    width = weights[0].shape[-1]
    for index, weight in enumerate(weights):
        product = jnp.dot(scaled, weight[layer], preferred_element_type=F32)
        for k, out in enumerate(outs):
            for member in range(group):
                block = slice((k ^ member) * count, ((k ^ member) + 1) * count)
                rows = slice(member * count, (member + 1) * count)
                out[rows, index * width : (index + 1) * width] = product[block].astype(out.dtype)
    for k, out in enumerate(outs):
        for member in range(group):
            block = slice((k ^ member) * count, ((k ^ member) + 1) * count)
            rows = slice(member * count, (member + 1) * count)
            out[rows, 4 * width :] = tail[block].astype(out.dtype)


def project_first(n_tp, layer, *refs):
    parts, (order, gain), weights = refs[:n_tp], refs[n_tp : n_tp + 2], refs[n_tp + 2 : n_tp + 6]
    base_out, outs, slots = refs[n_tp + 6], refs[n_tp + 7 : -1], refs[-1]
    rows = parts[0].shape[0]
    for k, part in enumerate(parts):
        slots[k * rows : (k + 1) * rows, :] = part[...].astype(F32)
    base = jnp.dot(order[...], slots[...].astype(BF16), preferred_element_type=F32)
    base_out[...] = base.astype(BF16)
    finish_projection(base, gain, layer, weights, outs)


def project_next(n_tp, layer, *refs):
    held, parts = refs[0], refs[1:n_tp]
    gain, weights = refs[n_tp], refs[n_tp + 1 : n_tp + 5]
    base_out, outs = refs[n_tp + 5], refs[n_tp + 6 :]
    base = held[...]
    for part in parts:
        base = base + part[...].astype(F32)
    rounded = base.astype(BF16)
    base_out[...] = rounded
    finish_projection(rounded.astype(F32), gain, layer, weights, outs)


def recur(n_dp, layer, features, group, *refs):
    own, parts = refs[0], refs[1:n_dp]
    (bound_ref, head_gain), states = refs[n_dp : n_dp + 2], refs[n_dp + 2 : n_dp + 2 + group]
    normed, gates, left = refs[n_dp + 2 + group :]
    kept, heads, hd = states[0].shape[:3]
    seqs = group * kept
    width = heads * hd
    total = own[...]
    for part in parts:
        total = total + part[...].astype(F32)
    mean = jnp.sum(total[:, 4 * width :], axis=1, keepdims=True) / features
    factor = lax.rsqrt(mean + 1e-06)
    query, forget_pre, value, gate_pre = (
        total[:, index * width : (index + 1) * width] * factor for index in range(4)
    )
    bound = bound_ref[layer : layer + 1, :]
    forget = bound + (1.0 - bound) * jax.nn.sigmoid(forget_pre)
    keyvec = (1.0 - bound) * jax.nn.sigmoid(-forget_pre)
    for seq in range(kept):
        for index, vector in enumerate((forget, keyvec, value)):
            gates[seq, index : index + 1, :] = vector[seq : seq + 1]
    gate = jax.nn.sigmoid(gate_pre)
    weighted = query * forget
    shared = query * keyvec
    row = lax.broadcasted_iota(jnp.int32, (seqs, hd), 0)
    terms = [term.astype(F32) for term in split(weighted)]
    wide = 2 if heads % 2 == 0 else 1
    for first in range(0, heads, wide):
        for index in range(wide):
            cols = slice((first + index) * hd, (first + index + 1) * hd)
            for part, term in enumerate(terms):
                top = (index * 2 + part) * seqs
                for seq in range(seqs):
                    left[top : top + seqs, seq * hd : (seq + 1) * hd] = jnp.where(
                        row == seq, term[:, cols], 0.0
                    )
        right = jnp.concatenate(
            [
                jnp.concatenate(
                    [
                        states[seq // kept][seq % kept, first + index]
                        for seq in range(seqs)
                    ],
                    axis=0,
                )
                for index in range(wide)
            ],
            axis=1,
        )
        product = jnp.dot(
            left[: 2 * wide * seqs, :].astype(BF16), right, preferred_element_type=F32
        )
        for index in range(wide):
            head = first + index
            cols = slice(head * hd, (head + 1) * hd)
            own_cols = slice(index * hd, (index + 1) * hd)
            readout = jnp.sum(shared[:, cols], axis=1, keepdims=True) * value[:, cols]
            for part in range(2):
                top = (index * 2 + part) * seqs
                readout = readout + product[top : top + seqs, own_cols]
            scale = lax.rsqrt(jnp.mean(readout * readout, axis=1, keepdims=True) + 1e-06)
            normed[:, cols] = (
                readout * scale * head_gain[layer : layer + 1, :] * gate[:, cols]
            ).astype(BF16)


def update(layer, gates, state, *refs):
    out, staged, sems = refs[-3:]
    seqs, heads, hd = state.shape[1], state.shape[2], state.shape[3]
    copies = []
    for seq in range(seqs):
        for head in range(heads):
            cols = slice(head * hd, (head + 1) * hd)
            forget, keyvec, value = (gates[seq, index : index + 1, cols] for index in range(3))
            forget = jnp.transpose(jnp.broadcast_to(forget, (hd, hd)))
            keyvec = jnp.transpose(jnp.broadcast_to(keyvec, (hd, hd)))
            staged[seq, head] = forget * state[layer, seq, head] + keyvec * value
        copies.append(pltpu.make_async_copy(staged.at[seq], out.at[layer, seq], sems.at[seq]))
        copies[-1].start()
    for copy in copies:
        copy.wait()


def narrow(layer, state, out, staged, sems):
    copies = [
        pltpu.make_async_copy(state.at[layer, seq], staged.at[seq], sems.at[seq])
        for seq in range(state.shape[1])
    ]
    for copy in copies:
        copy.start()
    for seq, copy in enumerate(copies):
        copy.wait()
        out[seq] = staged[seq].astype(BF16)


def slot_parts(refs, group):
    count = refs[0].shape[0] // group
    if group == 1:
        return [(ref, 0, count) for ref in refs]
    parts = [(refs[0], 0, count), (refs[0], count, count)]
    for ref in refs[1:]:
        parts += [(ref, count, count), (ref, 0, count)]
    return parts


def gather_rows(parts, slots):
    for k, (ref, top, count) in enumerate(parts):
        slots[k * count : (k + 1) * count, :] = ref[top : top + count, :].astype(F32)
    return slots[...].astype(BF16)


def mix_next(n_chip, group, layer, *refs):
    parts, (crossed, sent, slots) = slot_parts(refs[:n_chip], group), refs[n_chip:]
    facing = [parts[k ^ (group - 1)] for k in range(len(parts))]
    rows = gather_rows(facing, slots)
    sent[...] = jnp.dot(rows, crossed[layer], preferred_element_type=F32).astype(BF16)


def own_next(n_chip, group, layer, *refs):
    parts, (weight, base, held, slots) = slot_parts(refs[:n_chip], group), refs[n_chip:]
    rows = gather_rows(parts, slots)
    held[...] = base[...].astype(F32) + jnp.dot(rows, weight[layer], preferred_element_type=F32)


def mix_last(n_chip, group, layer, *refs):
    parts, (crossed, order) = slot_parts(refs[:n_chip], group), refs[n_chip : n_chip + 2]
    outs, slots = refs[n_chip + 2 : -1], refs[-1]
    rows = outs[0].shape[0]
    moved = jnp.dot(order[...], gather_rows(parts, slots), preferred_element_type=F32)
    product = jnp.dot(moved.astype(BF16), crossed[layer], preferred_element_type=F32)
    for k, out in enumerate(outs):
        out[...] = product[(k + 1) * rows : (k + 2) * rows].astype(BF16)


def own_last(n_chip, group, layer, *refs):
    parts, (weight, base, order, own, slots) = slot_parts(refs[:n_chip], group), refs[n_chip:]
    rows = own.shape[0]
    moved = jnp.dot(order[...], gather_rows(parts, slots), preferred_element_type=F32)
    own[...] = jnp.dot(moved.astype(BF16), weight[layer], preferred_element_type=F32)[
        :rows
    ] + jnp.dot(order[:rows, :], base[...], preferred_element_type=F32)


def close(own, *refs):
    total = own[...]
    for part in refs[:-1]:
        total = total + part[...].astype(F32)
    refs[-1][...] = total.astype(BF16)


def in_vmem(array):
    return pltpu.with_memory_space_constraint(array, pltpu.VMEM)


def stage(n_tp, n_dp, order_in, order_out):
    total = order_in.shape[0]

    def held(dim, n, index):
        row = lax.broadcasted_iota(jnp.int32, (total, total), dim)
        size = total // n
        return peer_of(n, row // size, index) * size + row % size

    tp, dp = lax.axis_index("tp"), lax.axis_index("dp")
    order_in[...] = jnp.where(held(0, n_dp, dp) == held(1, n_tp, tp), 1.0, 0.0).astype(BF16)
    order_out[...] = jnp.where(held(0, n_tp, tp) == held(1, n_dp, dp), 1.0, 0.0).astype(BF16)


def call(body, args, in_specs, outs, scratch=(), flops=None):
    return pl.pallas_call(
        body,
        out_shape=[pltpu.VMEM(shape, dtype) for shape, dtype in outs],
        in_specs=in_specs,
        out_specs=[VMEM] * len(outs),
        scratch_shapes=[pltpu.VMEM(shape, dtype) for shape, dtype in scratch],
        compiler_params=pltpu.CompilerParams(vmem_limit_bytes=8 << 20),
        cost_estimate=flops and pl.CostEstimate(flops=flops, bytes_accessed=0, transcendentals=0),
    )(*map(in_vmem, args))


def per_device(
    n_tp,
    n_dp,
    tokens,
    norm_gain,
    w_query,
    w_forget,
    w_value,
    w_gate,
    lower_bound,
    head_gain,
    w_out,
    state,
):
    seqs, heads, hd = state.shape[1], state.shape[2], state.shape[3]
    rows, local = tokens.shape
    features = local * n_dp
    total = rows * n_tp
    width = heads * hd
    weights = (w_query, w_forget, w_value, w_gate)
    order_in, order_out = call(
        functools.partial(stage, n_tp, n_dp),
        (),
        [],
        [((total, total), BF16)] * 2,
        flops=20_000_000_000,
    )
    parts = gather("tp", n_tp, tokens)
    flip = core_flip(n_dp)
    group, n_chip = flip + 1, n_dp // (flip + 1)
    crossed = cross_copy(n_dp, w_out)
    states = []
    for layer in range(2):
        narrowed = pl.pallas_call(
            functools.partial(narrow, layer),
            name="narrow",
            out_shape=pltpu.VMEM(state.shape[1:], BF16),
            in_specs=[ANY],
            out_specs=VMEM,
            scratch_shapes=[
                pltpu.VMEM(state.shape[1:], F32),
                pltpu.SemaphoreType.DMA((seqs,)),
            ],
            compiler_params=pltpu.CompilerParams(vmem_limit_bytes=4 << 20),
        )(pltpu.with_memory_space_constraint(state, pltpu.HBM))
        states.append([narrowed] + [cross_copy(n_dp, narrowed)] * flip)
    base = held = None
    new_state = None
    for layer in range(2):
        message = (group * seqs, 4 * width + LANES)
        outs = [((total, local), BF16), (message, F32)] + [(message, BF16)] * (n_dp - 1)
        specs = [VMEM] * 4
        if layer == 0:
            base, own, *sent = call(
                functools.partial(project_first, n_tp, layer),
                (*parts, order_in, norm_gain, *weights),
                [VMEM] * (n_tp + 2) + specs,
                outs,
                [((total, local), F32)],
            )
        else:
            base, own, *sent = call(
                functools.partial(project_next, n_tp, layer),
                (held, *parts, norm_gain, *weights),
                [VMEM] * (n_tp + 1) + specs,
                outs,
            )
        parts = exchange("dp", n_dp, sent)
        normed, gates = call(
            functools.partial(recur, n_dp, layer, features, group),
            (own, *parts, lower_bound, head_gain, *states[layer]),
            [VMEM] * (n_dp + 2 + group),
            [((group * seqs, width), BF16), ((seqs, 3, width), F32)],
            [((4 * group * seqs, group * seqs * hd), F32)],
        )
        read = gather("dp", n_dp, normed, chip_rounds(n_dp))
        slots = [((total, width), F32)]
        new_state = pl.pallas_call(
            functools.partial(update, layer),
            name="update",
            out_shape=jax.ShapeDtypeStruct(state.shape, F32),
            in_specs=[VMEM, VMEM] + ([ANY] if layer else []),
            out_specs=ANY,
            input_output_aliases={2: 0} if layer else {},
            scratch_shapes=[
                pltpu.VMEM((seqs, heads, hd, hd), F32),
                pltpu.SemaphoreType.DMA((seqs,)),
            ],
            compiler_params=pltpu.CompilerParams(vmem_limit_bytes=4 << 20),
        )(in_vmem(gates), in_vmem(state), *((new_state,) if layer else ()))
        if layer == 0:
            (sent,) = call(
                functools.partial(mix_next, n_chip, group, layer),
                (*read, crossed),
                [VMEM] * (n_chip + 1),
                [((total, local), BF16)],
                slots,
            )
            parts = cross_exchange(n_tp, n_dp, [sent] * (n_tp - 1))
            (held,) = call(
                functools.partial(own_next, n_chip, group, layer),
                (*read, w_out, base),
                [VMEM] * (n_chip + 2),
                [((total, local), F32)],
                slots,
            )
        else:
            sent = call(
                functools.partial(mix_last, n_chip, group, layer),
                (*read, crossed, order_out),
                [VMEM] * (n_chip + 2),
                [((rows, local), BF16)] * (n_tp - 1),
                slots,
            )
            parts = cross_exchange(n_tp, n_dp, sent)
            (own,) = call(
                functools.partial(own_last, n_chip, group, layer),
                (*read, w_out, base, order_out),
                [VMEM] * (n_chip + 3),
                [((rows, local), F32)],
                slots,
            )
    hidden = pl.pallas_call(
        close,
        name="close",
        out_shape=jax.ShapeDtypeStruct((rows, local), BF16),
        in_specs=[VMEM] * n_tp,
        out_specs=VMEM,
        compiler_params=pltpu.CompilerParams(vmem_limit_bytes=4 << 20),
    )(*map(in_vmem, (own, *parts)))
    return (hidden, new_state)


def solution(mesh):
    n_tp, n_dp = mesh.shape["tp"], mesh.shape["dp"]

    def body(*args):
        return per_device(n_tp, n_dp, *args)

    return jax.shard_map(
        body,
        mesh=mesh,
        in_specs=(
            P(("grp", "tp"), "dp"),
            P(None, "dp"),
            P(None, "dp", "tp"),
            P(None, "dp", "tp"),
            P(None, "dp", "tp"),
            P(None, "dp", "tp"),
            P(None, "tp"),
            P(),
            P(None, "tp", "dp"),
            P(None, ("grp", "dp"), "tp", None, None),
        ),
        out_specs=(P(("grp", "tp"), "dp"), P(None, ("grp", "dp"), "tp", None, None)),
        check_vma=False,
    )
```

```python
import functools

import jax
import jax.numpy as jnp
from jax import lax
from jax.experimental import pallas as pl
from jax.experimental.pallas import tpu as pltpu
from jax.sharding import PartitionSpec as P


F32, BF16 = jnp.float32, jnp.bfloat16
LANES = 128
VMEM = pl.BlockSpec(memory_space=pltpu.VMEM)
ANY = pl.BlockSpec(memory_space=pl.ANY)


def peer_of(n, k, index):
    if n & (n - 1) == 0:
        return index ^ k
    return (index + k) % n


def chip_rounds(n_dp):
    return list(range(3, n_dp, 2)) if core_flip(n_dp) else list(range(1, n_dp))


def exchange(axis, n, arrays, inward=False, rounds=None):
    rounds = rounds or list(range(1, n))
    parts = {}
    for k, array in reversed(list(zip(rounds, arrays))):
        pairs = [(i, peer_of(n, k, i)) for i in range(n)]
        parts[k] = lax.ppermute(array, axis, [(b, a) for a, b in pairs] if inward else pairs)
    return [parts[k] for k in rounds]


def core_flip(n_dp):
    return int(n_dp > 1 and n_dp & (n_dp - 1) == 0)


def cross_pairs(n_tp, n_dp, k):
    flip = core_flip(n_dp)
    return [
        (t * n_dp + d, peer_of(n_tp, k, t) * n_dp + (d ^ flip))
        for t in range(n_tp)
        for d in range(n_dp)
    ]


def cross_exchange(n_tp, n_dp, arrays):
    parts = [None] * (n_tp - 1)
    for k in reversed(range(1, n_tp)):
        parts[k - 1] = lax.ppermute(
            arrays[k - 1], ("tp", "dp"), cross_pairs(n_tp, n_dp, k)
        )
    return parts


def cross_copy(n_dp, array):
    if not core_flip(n_dp):
        return array
    return lax.ppermute(array, "dp", [(d, d ^ 1) for d in range(n_dp)])


def gather(axis, n, array, rounds=None):
    rounds = list(range(1, n)) if rounds is None else rounds
    if not rounds:
        return [array]
    return [array] + exchange(axis, n, [array] * len(rounds), True, rounds)


def split(array):
    high = array.astype(BF16)
    return high, (array - high.astype(F32)).astype(BF16)


def finish_projection(base, gain_ref, layer, weights, outs):
    count = base.shape[0] // len(outs)
    group = outs[0].shape[0] // count
    squares = jnp.sum(base * base, axis=1, keepdims=True)
    scaled = (base * gain_ref[layer : layer + 1, :]).astype(BF16)
    high, _ = split(squares)
    high = high.astype(F32)
    middle, low = split(squares - high)
    lane = lax.broadcasted_iota(jnp.int32, (base.shape[0], LANES), 1)
    zero = jnp.zeros((base.shape[0], LANES), F32)
    tail = jnp.where(lane == 0, high, zero)
    tail = jnp.where(lane == 1, middle.astype(F32), tail)
    tail = jnp.where(lane == 2, low.astype(F32), tail)
    width = weights[0].shape[-1]
    for index, weight in enumerate(weights):
        product = jnp.dot(scaled, weight[layer], preferred_element_type=F32)
        for k, out in enumerate(outs):
            for member in range(group):
                block = slice((k ^ member) * count, ((k ^ member) + 1) * count)
                rows = slice(member * count, (member + 1) * count)
                out[rows, index * width : (index + 1) * width] = product[block].astype(out.dtype)
    for k, out in enumerate(outs):
        for member in range(group):
            block = slice((k ^ member) * count, ((k ^ member) + 1) * count)
            rows = slice(member * count, (member + 1) * count)
            out[rows, 4 * width :] = tail[block].astype(out.dtype)


def project_first(n_tp, layer, *refs):
    parts, (order, gain), weights = refs[:n_tp], refs[n_tp : n_tp + 2], refs[n_tp + 2 : n_tp + 6]
    base_out, outs, slots = refs[n_tp + 6], refs[n_tp + 7 : -1], refs[-1]
    rows = parts[0].shape[0]
    for k, part in enumerate(parts):
        slots[k * rows : (k + 1) * rows, :] = part[...].astype(F32)
    base = jnp.dot(order[...], slots[...].astype(BF16), preferred_element_type=F32)
    base_out[...] = base.astype(BF16)
    finish_projection(base, gain, layer, weights, outs)


def project_next(n_tp, layer, *refs):
    held, parts = refs[0], refs[1:n_tp]
    gain, weights = refs[n_tp], refs[n_tp + 1 : n_tp + 5]
    base_out, outs = refs[n_tp + 5], refs[n_tp + 6 :]
    base = held[...]
    for part in parts:
        base = base + part[...].astype(F32)
    rounded = base.astype(BF16)
    base_out[...] = rounded
    finish_projection(rounded.astype(F32), gain, layer, weights, outs)


def recur(n_dp, layer, features, group, *refs):
    own, parts = refs[0], refs[1:n_dp]
    (bound_ref, head_gain), states = refs[n_dp : n_dp + 2], refs[n_dp + 2 : n_dp + 2 + group]
    normed, gates, left = refs[n_dp + 2 + group :]
    kept, heads, hd = states[0].shape[:3]
    seqs = group * kept
    width = heads * hd
    total = own[...]
    for part in parts:
        total = total + part[...].astype(F32)
    mean = jnp.sum(total[:, 4 * width :], axis=1, keepdims=True) / features
    factor = lax.rsqrt(mean + 1e-06)
    query, forget_pre, value, gate_pre = (
        total[:, index * width : (index + 1) * width] * factor for index in range(4)
    )
    bound = bound_ref[layer : layer + 1, :]
    forget = bound + (1.0 - bound) * jax.nn.sigmoid(forget_pre)
    keyvec = (1.0 - bound) * jax.nn.sigmoid(-forget_pre)
    for seq in range(kept):
        for index, vector in enumerate((forget, keyvec, value)):
            gates[seq, index : index + 1, :] = vector[seq : seq + 1]
    gate = jax.nn.sigmoid(gate_pre)
    weighted = query * forget
    shared = query * keyvec
    row = lax.broadcasted_iota(jnp.int32, (seqs, hd), 0)
    terms = [term.astype(F32) for term in split(weighted)]
    wide = 2 if heads % 2 == 0 else 1
    for first in range(0, heads, wide):
        for index in range(wide):
            cols = slice((first + index) * hd, (first + index + 1) * hd)
            for part, term in enumerate(terms):
                top = (index * 2 + part) * seqs
                for seq in range(seqs):
                    left[top : top + seqs, seq * hd : (seq + 1) * hd] = jnp.where(
                        row == seq, term[:, cols], 0.0
                    )
        right = jnp.concatenate(
            [
                jnp.concatenate(
                    [
                        states[seq // kept][seq % kept, first + index]
                        for seq in range(seqs)
                    ],
                    axis=0,
                )
                for index in range(wide)
            ],
            axis=1,
        )
        product = jnp.dot(
            left[: 2 * wide * seqs, :].astype(BF16), right, preferred_element_type=F32
        )
        for index in range(wide):
            head = first + index
            cols = slice(head * hd, (head + 1) * hd)
            own_cols = slice(index * hd, (index + 1) * hd)
            readout = jnp.sum(shared[:, cols], axis=1, keepdims=True) * value[:, cols]
            for part in range(2):
                top = (index * 2 + part) * seqs
                readout = readout + product[top : top + seqs, own_cols]
            scale = lax.rsqrt(jnp.mean(readout * readout, axis=1, keepdims=True) + 1e-06)
            normed[:, cols] = (
                readout * scale * head_gain[layer : layer + 1, :] * gate[:, cols]
            ).astype(BF16)


def update(layer, gates, state, *refs):
    out, staged, sems = refs[-3:]
    seqs, heads, hd = state.shape[1], state.shape[2], state.shape[3]
    copies = []
    for seq in range(seqs):
        for head in range(heads):
            cols = slice(head * hd, (head + 1) * hd)
            forget, keyvec, value = (gates[seq, index : index + 1, cols] for index in range(3))
            forget = jnp.transpose(jnp.broadcast_to(forget, (hd, hd)))
            keyvec = jnp.transpose(jnp.broadcast_to(keyvec, (hd, hd)))
            staged[seq, head] = forget * state[layer, seq, head] + keyvec * value
        copies.append(pltpu.make_async_copy(staged.at[seq], out.at[layer, seq], sems.at[seq]))
        copies[-1].start()
    for copy in copies:
        copy.wait()


def narrow(layer, state, out):
    out[...] = state[layer].astype(BF16)


def slot_parts(refs, group):
    count = refs[0].shape[0] // group
    if group == 1:
        return [(ref, 0, count) for ref in refs]
    parts = [(refs[0], 0, count), (refs[0], count, count)]
    for ref in refs[1:]:
        parts += [(ref, count, count), (ref, 0, count)]
    return parts


def gather_rows(parts, slots):
    for k, (ref, top, count) in enumerate(parts):
        slots[k * count : (k + 1) * count, :] = ref[top : top + count, :].astype(F32)
    return slots[...].astype(BF16)


def mix_next(n_chip, group, layer, *refs):
    parts, (crossed, sent, slots) = slot_parts(refs[:n_chip], group), refs[n_chip:]
    facing = [parts[k ^ (group - 1)] for k in range(len(parts))]
    rows = gather_rows(facing, slots)
    sent[...] = jnp.dot(rows, crossed[layer], preferred_element_type=F32).astype(BF16)


def own_next(n_chip, group, layer, *refs):
    parts, (weight, base, held, slots) = slot_parts(refs[:n_chip], group), refs[n_chip:]
    rows = gather_rows(parts, slots)
    held[...] = base[...].astype(F32) + jnp.dot(rows, weight[layer], preferred_element_type=F32)


def mix_last(n_chip, group, layer, *refs):
    parts, (crossed, order) = slot_parts(refs[:n_chip], group), refs[n_chip : n_chip + 2]
    outs, slots = refs[n_chip + 2 : -1], refs[-1]
    rows = outs[0].shape[0]
    moved = jnp.dot(order[...], gather_rows(parts, slots), preferred_element_type=F32)
    product = jnp.dot(moved.astype(BF16), crossed[layer], preferred_element_type=F32)
    for k, out in enumerate(outs):
        out[...] = product[(k + 1) * rows : (k + 2) * rows].astype(BF16)


def own_last(n_chip, group, layer, *refs):
    parts, (weight, base, order, own, slots) = slot_parts(refs[:n_chip], group), refs[n_chip:]
    rows = own.shape[0]
    moved = jnp.dot(order[...], gather_rows(parts, slots), preferred_element_type=F32)
    own[...] = jnp.dot(moved.astype(BF16), weight[layer], preferred_element_type=F32)[
        :rows
    ] + jnp.dot(order[:rows, :], base[...], preferred_element_type=F32)


def close(own, *refs):
    total = own[...]
    for part in refs[:-1]:
        total = total + part[...].astype(F32)
    refs[-1][...] = total.astype(BF16)


def in_vmem(array):
    return pltpu.with_memory_space_constraint(array, pltpu.VMEM)


def stage(n_tp, n_dp, order_in, order_out):
    total = order_in.shape[0]

    def held(dim, n, index):
        row = lax.broadcasted_iota(jnp.int32, (total, total), dim)
        size = total // n
        return peer_of(n, row // size, index) * size + row % size

    tp, dp = lax.axis_index("tp"), lax.axis_index("dp")
    order_in[...] = jnp.where(held(0, n_dp, dp) == held(1, n_tp, tp), 1.0, 0.0).astype(BF16)
    order_out[...] = jnp.where(held(0, n_tp, tp) == held(1, n_dp, dp), 1.0, 0.0).astype(BF16)


def call(body, args, in_specs, outs, scratch=(), flops=None):
    return pl.pallas_call(
        body,
        out_shape=[pltpu.VMEM(shape, dtype) for shape, dtype in outs],
        in_specs=in_specs,
        out_specs=[VMEM] * len(outs),
        scratch_shapes=[pltpu.VMEM(shape, dtype) for shape, dtype in scratch],
        compiler_params=pltpu.CompilerParams(vmem_limit_bytes=8 << 20),
        cost_estimate=flops and pl.CostEstimate(flops=flops, bytes_accessed=0, transcendentals=0),
    )(*map(in_vmem, args))


def per_device(
    n_tp,
    n_dp,
    tokens,
    norm_gain,
    w_query,
    w_forget,
    w_value,
    w_gate,
    lower_bound,
    head_gain,
    w_out,
    state,
):
    seqs, heads, hd = state.shape[1], state.shape[2], state.shape[3]
    rows, local = tokens.shape
    features = local * n_dp
    total = rows * n_tp
    width = heads * hd
    weights = (w_query, w_forget, w_value, w_gate)
    order_in, order_out = call(
        functools.partial(stage, n_tp, n_dp),
        (),
        [],
        [((total, total), BF16)] * 2,
        flops=20_000_000_000,
    )
    parts = gather("tp", n_tp, tokens)
    flip = core_flip(n_dp)
    group, n_chip = flip + 1, n_dp // (flip + 1)
    crossed = cross_copy(n_dp, w_out)
    states = []
    for layer in range(2):
        (narrowed,) = call(
            functools.partial(narrow, layer), (state,), [VMEM], [(state.shape[1:], BF16)]
        )
        states.append([narrowed] + [cross_copy(n_dp, narrowed)] * flip)
    base = held = None
    new_state = None
    for layer in range(2):
        message = (group * seqs, 4 * width + LANES)
        outs = [((total, local), BF16), (message, F32)] + [(message, BF16)] * (n_dp - 1)
        specs = [VMEM] * 4
        if layer == 0:
            base, own, *sent = call(
                functools.partial(project_first, n_tp, layer),
                (*parts, order_in, norm_gain, *weights),
                [VMEM] * (n_tp + 2) + specs,
                outs,
                [((total, local), F32)],
            )
        else:
            base, own, *sent = call(
                functools.partial(project_next, n_tp, layer),
                (held, *parts, norm_gain, *weights),
                [VMEM] * (n_tp + 1) + specs,
                outs,
            )
        parts = exchange("dp", n_dp, sent)
        normed, gates = call(
            functools.partial(recur, n_dp, layer, features, group),
            (own, *parts, lower_bound, head_gain, *states[layer]),
            [VMEM] * (n_dp + 2 + group),
            [((group * seqs, width), BF16), ((seqs, 3, width), F32)],
            [((4 * group * seqs, group * seqs * hd), F32)],
        )
        read = gather("dp", n_dp, normed, chip_rounds(n_dp))
        slots = [((total, width), F32)]
        new_state = pl.pallas_call(
            functools.partial(update, layer),
            name="update",
            out_shape=jax.ShapeDtypeStruct(state.shape, F32),
            in_specs=[VMEM, VMEM] + ([ANY] if layer else []),
            out_specs=ANY,
            input_output_aliases={2: 0} if layer else {},
            scratch_shapes=[
                pltpu.VMEM((seqs, heads, hd, hd), F32),
                pltpu.SemaphoreType.DMA((seqs,)),
            ],
            compiler_params=pltpu.CompilerParams(vmem_limit_bytes=4 << 20),
        )(in_vmem(gates), in_vmem(state), *((new_state,) if layer else ()))
        if layer == 0:
            (sent,) = call(
                functools.partial(mix_next, n_chip, group, layer),
                (*read, crossed),
                [VMEM] * (n_chip + 1),
                [((total, local), BF16)],
                slots,
            )
            parts = cross_exchange(n_tp, n_dp, [sent] * (n_tp - 1))
            (held,) = call(
                functools.partial(own_next, n_chip, group, layer),
                (*read, w_out, base),
                [VMEM] * (n_chip + 2),
                [((total, local), F32)],
                slots,
            )
        else:
            sent = call(
                functools.partial(mix_last, n_chip, group, layer),
                (*read, crossed, order_out),
                [VMEM] * (n_chip + 2),
                [((rows, local), BF16)] * (n_tp - 1),
                slots,
            )
            parts = cross_exchange(n_tp, n_dp, sent)
            (own,) = call(
                functools.partial(own_last, n_chip, group, layer),
                (*read, w_out, base, order_out),
                [VMEM] * (n_chip + 3),
                [((rows, local), F32)],
                slots,
            )
    hidden = pl.pallas_call(
        close,
        name="close",
        out_shape=jax.ShapeDtypeStruct((rows, local), BF16),
        in_specs=[VMEM] * n_tp,
        out_specs=VMEM,
        compiler_params=pltpu.CompilerParams(vmem_limit_bytes=4 << 20),
    )(*map(in_vmem, (own, *parts)))
    return (hidden, new_state)


def solution(mesh):
    n_tp, n_dp = mesh.shape["tp"], mesh.shape["dp"]

    def body(*args):
        return per_device(n_tp, n_dp, *args)

    return jax.shard_map(
        body,
        mesh=mesh,
        in_specs=(
            P(("grp", "tp"), "dp"),
            P(None, "dp"),
            P(None, "dp", "tp"),
            P(None, "dp", "tp"),
            P(None, "dp", "tp"),
            P(None, "dp", "tp"),
            P(None, "tp"),
            P(),
            P(None, "tp", "dp"),
            P(None, ("grp", "dp"), "tp", None, None),
        ),
        out_specs=(P(("grp", "tp"), "dp"), P(None, ("grp", "dp"), "tp", None, None)),
        check_vma=False,
    )
```

```python
import functools

import jax
import jax.numpy as jnp
from jax import lax
from jax.experimental import pallas as pl
from jax.experimental.pallas import tpu as pltpu
from jax.sharding import PartitionSpec as P


F32, BF16 = jnp.float32, jnp.bfloat16
LANES = 128
VMEM = pl.BlockSpec(memory_space=pltpu.VMEM)
ANY = pl.BlockSpec(memory_space=pl.ANY)


def peer_of(n, k, index):
    if n & (n - 1) == 0:
        return index ^ k
    return (index + k) % n


def chip_rounds(n_dp):
    return list(range(3, n_dp, 2)) if core_flip(n_dp) else list(range(1, n_dp))


def start_order(axis, rounds):
    order = list(reversed(rounds))
    if axis == "tp" and len(order) > 2:
        order[:2] = order[1], order[0]
    return order


def exchange(axis, n, arrays, inward=False, rounds=None):
    rounds = rounds or list(range(1, n))
    held, parts = dict(zip(rounds, arrays)), {}
    for k in start_order(axis, rounds):
        array = held[k]
        pairs = [(i, peer_of(n, k, i)) for i in range(n)]
        parts[k] = lax.ppermute(array, axis, [(b, a) for a, b in pairs] if inward else pairs)
    return [parts[k] for k in rounds]


def core_flip(n_dp):
    return int(n_dp > 1 and n_dp & (n_dp - 1) == 0)


def cross_pairs(n_tp, n_dp, k):
    flip = core_flip(n_dp)
    return [
        (t * n_dp + d, peer_of(n_tp, k, t) * n_dp + (d ^ flip))
        for t in range(n_tp)
        for d in range(n_dp)
    ]


def cross_exchange(n_tp, n_dp, arrays):
    parts = [None] * (n_tp - 1)
    for k in start_order("tp", list(range(1, n_tp))):
        parts[k - 1] = lax.ppermute(
            arrays[k - 1], ("tp", "dp"), cross_pairs(n_tp, n_dp, k)
        )
    return parts


def cross_copy(n_dp, array):
    if not core_flip(n_dp):
        return array
    return lax.ppermute(array, "dp", [(d, d ^ 1) for d in range(n_dp)])


def gather(axis, n, array, rounds=None):
    rounds = list(range(1, n)) if rounds is None else rounds
    if not rounds:
        return [array]
    return [array] + exchange(axis, n, [array] * len(rounds), True, rounds)


def split(array):
    high = array.astype(BF16)
    return high, (array - high.astype(F32)).astype(BF16)


def finish_projection(base, gain_ref, layer, weights, outs):
    count = base.shape[0] // len(outs)
    group = outs[0].shape[0] // count
    squares = jnp.sum(base * base, axis=1, keepdims=True)
    scaled = (base * gain_ref[layer : layer + 1, :]).astype(BF16)
    high, _ = split(squares)
    high = high.astype(F32)
    middle, low = split(squares - high)
    lane = lax.broadcasted_iota(jnp.int32, (base.shape[0], LANES), 1)
    zero = jnp.zeros((base.shape[0], LANES), F32)
    tail = jnp.where(lane == 0, high, zero)
    tail = jnp.where(lane == 1, middle.astype(F32), tail)
    tail = jnp.where(lane == 2, low.astype(F32), tail)
    width = weights[0].shape[-1]
    for index, weight in enumerate(weights):
        product = jnp.dot(scaled, weight[layer], preferred_element_type=F32)
        for k, out in enumerate(outs):
            for member in range(group):
                block = slice((k ^ member) * count, ((k ^ member) + 1) * count)
                rows = slice(member * count, (member + 1) * count)
                out[rows, index * width : (index + 1) * width] = product[block].astype(out.dtype)
    for k, out in enumerate(outs):
        for member in range(group):
            block = slice((k ^ member) * count, ((k ^ member) + 1) * count)
            rows = slice(member * count, (member + 1) * count)
            out[rows, 4 * width :] = tail[block].astype(out.dtype)


def project_first(n_tp, layer, *refs):
    parts, (order, gain), weights = refs[:n_tp], refs[n_tp : n_tp + 2], refs[n_tp + 2 : n_tp + 6]
    base_out, outs, slots = refs[n_tp + 6], refs[n_tp + 7 : -1], refs[-1]
    rows = parts[0].shape[0]
    for k, part in enumerate(parts):
        slots[k * rows : (k + 1) * rows, :] = part[...].astype(F32)
    base = jnp.dot(order[...], slots[...].astype(BF16), preferred_element_type=F32)
    base_out[...] = base.astype(BF16)
    finish_projection(base, gain, layer, weights, outs)


def project_next(n_tp, layer, *refs):
    held, parts = refs[0], refs[1:n_tp]
    gain, weights = refs[n_tp], refs[n_tp + 1 : n_tp + 5]
    base_out, outs = refs[n_tp + 5], refs[n_tp + 6 :]
    base = held[...]
    for part in parts:
        base = base + part[...].astype(F32)
    rounded = base.astype(BF16)
    base_out[...] = rounded
    finish_projection(rounded.astype(F32), gain, layer, weights, outs)


def recur(n_dp, layer, features, group, *refs):
    own, parts = refs[0], refs[1:n_dp]
    (bound_ref, head_gain), states = refs[n_dp : n_dp + 2], refs[n_dp + 2 : n_dp + 2 + group]
    normed, gates, left = refs[n_dp + 2 + group :]
    kept, heads, hd = states[0].shape[:3]
    seqs = group * kept
    width = heads * hd
    total = own[...]
    for part in parts:
        total = total + part[...].astype(F32)
    mean = jnp.sum(total[:, 4 * width :], axis=1, keepdims=True) / features
    factor = lax.rsqrt(mean + 1e-06)
    query, forget_pre, value, gate_pre = (
        total[:, index * width : (index + 1) * width] * factor for index in range(4)
    )
    bound = bound_ref[layer : layer + 1, :]
    forget = bound + (1.0 - bound) * jax.nn.sigmoid(forget_pre)
    keyvec = (1.0 - bound) * jax.nn.sigmoid(-forget_pre)
    for seq in range(kept):
        for index, vector in enumerate((forget, keyvec, value)):
            gates[seq, index : index + 1, :] = vector[seq : seq + 1]
    gate = jax.nn.sigmoid(gate_pre)
    weighted = query * forget
    shared = query * keyvec
    row = lax.broadcasted_iota(jnp.int32, (seqs, hd), 0)
    terms = [term.astype(F32) for term in split(weighted)]
    wide = 2 if heads % 2 == 0 else 1
    for first in range(0, heads, wide):
        for index in range(wide):
            cols = slice((first + index) * hd, (first + index + 1) * hd)
            for part, term in enumerate(terms):
                top = (index * 2 + part) * seqs
                for seq in range(seqs):
                    left[top : top + seqs, seq * hd : (seq + 1) * hd] = jnp.where(
                        row == seq, term[:, cols], 0.0
                    )
        right = jnp.concatenate(
            [
                jnp.concatenate(
                    [
                        states[seq // kept][seq % kept, first + index]
                        for seq in range(seqs)
                    ],
                    axis=0,
                )
                for index in range(wide)
            ],
            axis=1,
        )
        product = jnp.dot(
            left[: 2 * wide * seqs, :].astype(BF16), right, preferred_element_type=F32
        )
        for index in range(wide):
            head = first + index
            cols = slice(head * hd, (head + 1) * hd)
            own_cols = slice(index * hd, (index + 1) * hd)
            readout = jnp.sum(shared[:, cols], axis=1, keepdims=True) * value[:, cols]
            for part in range(2):
                top = (index * 2 + part) * seqs
                readout = readout + product[top : top + seqs, own_cols]
            scale = lax.rsqrt(jnp.mean(readout * readout, axis=1, keepdims=True) + 1e-06)
            normed[:, cols] = (
                readout * scale * head_gain[layer : layer + 1, :] * gate[:, cols]
            ).astype(BF16)


def update(layer, gates, state, *refs):
    out, staged, sems = refs[-3:]
    seqs, heads, hd = state.shape[1], state.shape[2], state.shape[3]
    copies = []
    for seq in range(seqs):
        for head in range(heads):
            cols = slice(head * hd, (head + 1) * hd)
            forget, keyvec, value = (gates[seq, index : index + 1, cols] for index in range(3))
            forget = jnp.transpose(jnp.broadcast_to(forget, (hd, hd)))
            keyvec = jnp.transpose(jnp.broadcast_to(keyvec, (hd, hd)))
            staged[seq, head] = forget * state[layer, seq, head] + keyvec * value
        copies.append(pltpu.make_async_copy(staged.at[seq], out.at[layer, seq], sems.at[seq]))
        copies[-1].start()
    for copy in copies:
        copy.wait()


def narrow(layer, state, out):
    out[...] = state[layer].astype(BF16)


def slot_parts(refs, group):
    count = refs[0].shape[0] // group
    if group == 1:
        return [(ref, 0, count) for ref in refs]
    parts = [(refs[0], 0, count), (refs[0], count, count)]
    for ref in refs[1:]:
        parts += [(ref, count, count), (ref, 0, count)]
    return parts


def gather_rows(parts, slots):
    for k, (ref, top, count) in enumerate(parts):
        slots[k * count : (k + 1) * count, :] = ref[top : top + count, :].astype(F32)
    return slots[...].astype(BF16)


def mix_next(n_chip, group, layer, *refs):
    parts, (crossed, sent, slots) = slot_parts(refs[:n_chip], group), refs[n_chip:]
    facing = [parts[k ^ (group - 1)] for k in range(len(parts))]
    rows = gather_rows(facing, slots)
    sent[...] = jnp.dot(rows, crossed[layer], preferred_element_type=F32).astype(BF16)


def own_next(n_chip, group, layer, *refs):
    parts, (weight, base, held, slots) = slot_parts(refs[:n_chip], group), refs[n_chip:]
    rows = gather_rows(parts, slots)
    held[...] = base[...].astype(F32) + jnp.dot(rows, weight[layer], preferred_element_type=F32)


def mix_last(n_chip, group, layer, *refs):
    parts, (crossed, order) = slot_parts(refs[:n_chip], group), refs[n_chip : n_chip + 2]
    outs, slots = refs[n_chip + 2 : -1], refs[-1]
    rows = outs[0].shape[0]
    moved = jnp.dot(order[...], gather_rows(parts, slots), preferred_element_type=F32)
    product = jnp.dot(moved.astype(BF16), crossed[layer], preferred_element_type=F32)
    for k, out in enumerate(outs):
        out[...] = product[(k + 1) * rows : (k + 2) * rows].astype(BF16)


def own_last(n_chip, group, layer, *refs):
    parts, (weight, base, order, own, slots) = slot_parts(refs[:n_chip], group), refs[n_chip:]
    rows = own.shape[0]
    moved = jnp.dot(order[...], gather_rows(parts, slots), preferred_element_type=F32)
    own[...] = jnp.dot(moved.astype(BF16), weight[layer], preferred_element_type=F32)[
        :rows
    ] + jnp.dot(order[:rows, :], base[...], preferred_element_type=F32)


def close(own, *refs):
    total = own[...]
    for part in refs[:-1]:
        total = total + part[...].astype(F32)
    refs[-1][...] = total.astype(BF16)


def in_vmem(array):
    return pltpu.with_memory_space_constraint(array, pltpu.VMEM)


def stage(n_tp, n_dp, order_in, order_out):
    total = order_in.shape[0]

    def held(dim, n, index):
        row = lax.broadcasted_iota(jnp.int32, (total, total), dim)
        size = total // n
        return peer_of(n, row // size, index) * size + row % size

    tp, dp = lax.axis_index("tp"), lax.axis_index("dp")
    order_in[...] = jnp.where(held(0, n_dp, dp) == held(1, n_tp, tp), 1.0, 0.0).astype(BF16)
    order_out[...] = jnp.where(held(0, n_tp, tp) == held(1, n_dp, dp), 1.0, 0.0).astype(BF16)


def call(body, args, in_specs, outs, scratch=(), flops=None):
    return pl.pallas_call(
        body,
        out_shape=[pltpu.VMEM(shape, dtype) for shape, dtype in outs],
        in_specs=in_specs,
        out_specs=[VMEM] * len(outs),
        scratch_shapes=[pltpu.VMEM(shape, dtype) for shape, dtype in scratch],
        compiler_params=pltpu.CompilerParams(vmem_limit_bytes=8 << 20),
        cost_estimate=flops and pl.CostEstimate(flops=flops, bytes_accessed=0, transcendentals=0),
    )(*map(in_vmem, args))


def per_device(
    n_tp,
    n_dp,
    tokens,
    norm_gain,
    w_query,
    w_forget,
    w_value,
    w_gate,
    lower_bound,
    head_gain,
    w_out,
    state,
):
    seqs, heads, hd = state.shape[1], state.shape[2], state.shape[3]
    rows, local = tokens.shape
    features = local * n_dp
    total = rows * n_tp
    width = heads * hd
    weights = (w_query, w_forget, w_value, w_gate)
    order_in, order_out = call(
        functools.partial(stage, n_tp, n_dp),
        (),
        [],
        [((total, total), BF16)] * 2,
        flops=20_000_000_000,
    )
    parts = gather("tp", n_tp, tokens)
    flip = core_flip(n_dp)
    group, n_chip = flip + 1, n_dp // (flip + 1)
    crossed = cross_copy(n_dp, w_out)
    states = []
    for layer in range(2):
        (narrowed,) = call(
            functools.partial(narrow, layer), (state,), [VMEM], [(state.shape[1:], BF16)]
        )
        states.append([narrowed] + [cross_copy(n_dp, narrowed)] * flip)
    base = held = None
    new_state = None
    for layer in range(2):
        message = (group * seqs, 4 * width + LANES)
        outs = [((total, local), BF16), (message, F32)] + [(message, BF16)] * (n_dp - 1)
        specs = [VMEM] * 4
        if layer == 0:
            base, own, *sent = call(
                functools.partial(project_first, n_tp, layer),
                (*parts, order_in, norm_gain, *weights),
                [VMEM] * (n_tp + 2) + specs,
                outs,
                [((total, local), F32)],
            )
        else:
            base, own, *sent = call(
                functools.partial(project_next, n_tp, layer),
                (held, *parts, norm_gain, *weights),
                [VMEM] * (n_tp + 1) + specs,
                outs,
            )
        parts = exchange("dp", n_dp, sent)
        normed, gates = call(
            functools.partial(recur, n_dp, layer, features, group),
            (own, *parts, lower_bound, head_gain, *states[layer]),
            [VMEM] * (n_dp + 2 + group),
            [((group * seqs, width), BF16), ((seqs, 3, width), F32)],
            [((4 * group * seqs, group * seqs * hd), F32)],
        )
        read = gather("dp", n_dp, normed, chip_rounds(n_dp))
        slots = [((total, width), F32)]
        new_state = pl.pallas_call(
            functools.partial(update, layer),
            name="update",
            out_shape=jax.ShapeDtypeStruct(state.shape, F32),
            in_specs=[VMEM, VMEM] + ([ANY] if layer else []),
            out_specs=ANY,
            input_output_aliases={2: 0} if layer else {},
            scratch_shapes=[
                pltpu.VMEM((seqs, heads, hd, hd), F32),
                pltpu.SemaphoreType.DMA((seqs,)),
            ],
            compiler_params=pltpu.CompilerParams(vmem_limit_bytes=4 << 20),
        )(in_vmem(gates), in_vmem(state), *((new_state,) if layer else ()))
        if layer == 0:
            (sent,) = call(
                functools.partial(mix_next, n_chip, group, layer),
                (*read, crossed),
                [VMEM] * (n_chip + 1),
                [((total, local), BF16)],
                slots,
            )
            parts = cross_exchange(n_tp, n_dp, [sent] * (n_tp - 1))
            (held,) = call(
                functools.partial(own_next, n_chip, group, layer),
                (*read, w_out, base),
                [VMEM] * (n_chip + 2),
                [((total, local), F32)],
                slots,
            )
        else:
            sent = call(
                functools.partial(mix_last, n_chip, group, layer),
                (*read, crossed, order_out),
                [VMEM] * (n_chip + 2),
                [((rows, local), BF16)] * (n_tp - 1),
                slots,
            )
            parts = cross_exchange(n_tp, n_dp, sent)
            (own,) = call(
                functools.partial(own_last, n_chip, group, layer),
                (*read, w_out, base, order_out),
                [VMEM] * (n_chip + 3),
                [((rows, local), F32)],
                slots,
            )
    hidden = pl.pallas_call(
        close,
        name="close",
        out_shape=jax.ShapeDtypeStruct((rows, local), BF16),
        in_specs=[VMEM] * n_tp,
        out_specs=VMEM,
        compiler_params=pltpu.CompilerParams(vmem_limit_bytes=4 << 20),
    )(*map(in_vmem, (own, *parts)))
    return (hidden, new_state)


def solution(mesh):
    n_tp, n_dp = mesh.shape["tp"], mesh.shape["dp"]

    def body(*args):
        return per_device(n_tp, n_dp, *args)

    return jax.shard_map(
        body,
        mesh=mesh,
        in_specs=(
            P(("grp", "tp"), "dp"),
            P(None, "dp"),
            P(None, "dp", "tp"),
            P(None, "dp", "tp"),
            P(None, "dp", "tp"),
            P(None, "dp", "tp"),
            P(None, "tp"),
            P(),
            P(None, "tp", "dp"),
            P(None, ("grp", "dp"), "tp", None, None),
        ),
        out_specs=(P(("grp", "tp"), "dp"), P(None, ("grp", "dp"), "tp", None, None)),
        check_vma=False,
    )
```

```python
import functools

import jax
import jax.numpy as jnp
from jax import lax
from jax.experimental import pallas as pl
from jax.experimental.pallas import tpu as pltpu
from jax.sharding import PartitionSpec as P


F32, BF16 = jnp.float32, jnp.bfloat16
LANES = 128
VMEM = pl.BlockSpec(memory_space=pltpu.VMEM)
ANY = pl.BlockSpec(memory_space=pl.ANY)


def peer_of(n, k, index):
    if n & (n - 1) == 0:
        return index ^ k
    return (index + k) % n


def chip_rounds(n_dp):
    return list(range(3, n_dp, 2)) if core_flip(n_dp) else list(range(1, n_dp))


def start_order(tag, rounds):
    order = list(reversed(rounds))
    if tag in "ade" and len(order) > 2:
        order[:2] = order[1], order[0]
    return order


def exchange(tag, axis, n, arrays, inward=False, rounds=None):
    rounds = rounds or list(range(1, n))
    held, parts = dict(zip(rounds, arrays)), {}
    for k in start_order(tag, rounds):
        array = held[k]
        pairs = [(i, peer_of(n, k, i)) for i in range(n)]
        parts[k] = lax.ppermute(array, axis, [(b, a) for a, b in pairs] if inward else pairs)
    return [parts[k] for k in rounds]


def core_flip(n_dp):
    return int(n_dp > 1 and n_dp & (n_dp - 1) == 0)


def cross_pairs(n_tp, n_dp, k):
    flip = core_flip(n_dp)
    return [
        (t * n_dp + d, peer_of(n_tp, k, t) * n_dp + (d ^ flip))
        for t in range(n_tp)
        for d in range(n_dp)
    ]


def cross_exchange(tag, n_tp, n_dp, arrays):
    parts = [None] * (n_tp - 1)
    for k in start_order(tag, list(range(1, n_tp))):
        parts[k - 1] = lax.ppermute(
            arrays[k - 1], ("tp", "dp"), cross_pairs(n_tp, n_dp, k)
        )
    return parts


def cross_copy(n_dp, array):
    if not core_flip(n_dp):
        return array
    return lax.ppermute(array, "dp", [(d, d ^ 1) for d in range(n_dp)])


def gather(tag, axis, n, array, rounds=None):
    rounds = list(range(1, n)) if rounds is None else rounds
    if not rounds:
        return [array]
    return [array] + exchange(tag, axis, n, [array] * len(rounds), True, rounds)


def split(array):
    high = array.astype(BF16)
    return high, (array - high.astype(F32)).astype(BF16)


def finish_projection(base, gain_ref, layer, weights, outs):
    count = base.shape[0] // len(outs)
    group = outs[0].shape[0] // count
    squares = jnp.sum(base * base, axis=1, keepdims=True)
    scaled = (base * gain_ref[layer : layer + 1, :]).astype(BF16)
    high, _ = split(squares)
    high = high.astype(F32)
    middle, low = split(squares - high)
    lane = lax.broadcasted_iota(jnp.int32, (base.shape[0], LANES), 1)
    zero = jnp.zeros((base.shape[0], LANES), F32)
    tail = jnp.where(lane == 0, high, zero)
    tail = jnp.where(lane == 1, middle.astype(F32), tail)
    tail = jnp.where(lane == 2, low.astype(F32), tail)
    width = weights[0].shape[-1]
    for index, weight in enumerate(weights):
        product = jnp.dot(scaled, weight[layer], preferred_element_type=F32)
        for k, out in enumerate(outs):
            for member in range(group):
                block = slice((k ^ member) * count, ((k ^ member) + 1) * count)
                rows = slice(member * count, (member + 1) * count)
                out[rows, index * width : (index + 1) * width] = product[block].astype(out.dtype)
    for k, out in enumerate(outs):
        for member in range(group):
            block = slice((k ^ member) * count, ((k ^ member) + 1) * count)
            rows = slice(member * count, (member + 1) * count)
            out[rows, 4 * width :] = tail[block].astype(out.dtype)


def project_first(n_tp, layer, *refs):
    parts, (order, gain), weights = refs[:n_tp], refs[n_tp : n_tp + 2], refs[n_tp + 2 : n_tp + 6]
    base_out, outs, slots = refs[n_tp + 6], refs[n_tp + 7 : -1], refs[-1]
    rows = parts[0].shape[0]
    for k, part in enumerate(parts):
        slots[k * rows : (k + 1) * rows, :] = part[...].astype(F32)
    base = jnp.dot(order[...], slots[...].astype(BF16), preferred_element_type=F32)
    base_out[...] = base.astype(BF16)
    finish_projection(base, gain, layer, weights, outs)


def project_next(n_tp, layer, *refs):
    held, parts = refs[0], refs[1:n_tp]
    gain, weights = refs[n_tp], refs[n_tp + 1 : n_tp + 5]
    base_out, outs = refs[n_tp + 5], refs[n_tp + 6 :]
    base = held[...]
    for part in parts:
        base = base + part[...].astype(F32)
    rounded = base.astype(BF16)
    base_out[...] = rounded
    finish_projection(rounded.astype(F32), gain, layer, weights, outs)


def recur(n_dp, layer, features, group, *refs):
    own, parts = refs[0], refs[1:n_dp]
    (bound_ref, head_gain), states = refs[n_dp : n_dp + 2], refs[n_dp + 2 : n_dp + 2 + group]
    normed, gates, left = refs[n_dp + 2 + group :]
    kept, heads, hd = states[0].shape[:3]
    seqs = group * kept
    width = heads * hd
    total = own[...]
    for part in parts:
        total = total + part[...].astype(F32)
    mean = jnp.sum(total[:, 4 * width :], axis=1, keepdims=True) / features
    factor = lax.rsqrt(mean + 1e-06)
    query, forget_pre, value, gate_pre = (
        total[:, index * width : (index + 1) * width] * factor for index in range(4)
    )
    bound = bound_ref[layer : layer + 1, :]
    forget = bound + (1.0 - bound) * jax.nn.sigmoid(forget_pre)
    keyvec = (1.0 - bound) * jax.nn.sigmoid(-forget_pre)
    for seq in range(kept):
        for index, vector in enumerate((forget, keyvec, value)):
            gates[seq, index : index + 1, :] = vector[seq : seq + 1]
    gate = jax.nn.sigmoid(gate_pre)
    weighted = query * forget
    shared = query * keyvec
    row = lax.broadcasted_iota(jnp.int32, (seqs, hd), 0)
    terms = [term.astype(F32) for term in split(weighted)]
    wide = 2 if heads % 2 == 0 else 1
    for first in range(0, heads, wide):
        for index in range(wide):
            cols = slice((first + index) * hd, (first + index + 1) * hd)
            for part, term in enumerate(terms):
                top = (index * 2 + part) * seqs
                for seq in range(seqs):
                    left[top : top + seqs, seq * hd : (seq + 1) * hd] = jnp.where(
                        row == seq, term[:, cols], 0.0
                    )
        right = jnp.concatenate(
            [
                jnp.concatenate(
                    [
                        states[seq // kept][seq % kept, first + index]
                        for seq in range(seqs)
                    ],
                    axis=0,
                )
                for index in range(wide)
            ],
            axis=1,
        )
        product = jnp.dot(
            left[: 2 * wide * seqs, :].astype(BF16), right, preferred_element_type=F32
        )
        for index in range(wide):
            head = first + index
            cols = slice(head * hd, (head + 1) * hd)
            own_cols = slice(index * hd, (index + 1) * hd)
            readout = jnp.sum(shared[:, cols], axis=1, keepdims=True) * value[:, cols]
            for part in range(2):
                top = (index * 2 + part) * seqs
                readout = readout + product[top : top + seqs, own_cols]
            scale = lax.rsqrt(jnp.mean(readout * readout, axis=1, keepdims=True) + 1e-06)
            normed[:, cols] = (
                readout * scale * head_gain[layer : layer + 1, :] * gate[:, cols]
            ).astype(BF16)


def update(layer, gates, state, *refs):
    out, staged, sems = refs[-3:]
    seqs, heads, hd = state.shape[1], state.shape[2], state.shape[3]
    copies = []
    for seq in range(seqs):
        for head in range(heads):
            cols = slice(head * hd, (head + 1) * hd)
            forget, keyvec, value = (gates[seq, index : index + 1, cols] for index in range(3))
            forget = jnp.transpose(jnp.broadcast_to(forget, (hd, hd)))
            keyvec = jnp.transpose(jnp.broadcast_to(keyvec, (hd, hd)))
            staged[seq, head] = forget * state[layer, seq, head] + keyvec * value
        copies.append(pltpu.make_async_copy(staged.at[seq], out.at[layer, seq], sems.at[seq]))
        copies[-1].start()
    for copy in copies:
        copy.wait()


def narrow(layer, state, out):
    out[...] = state[layer].astype(BF16)


def slot_parts(refs, group):
    count = refs[0].shape[0] // group
    if group == 1:
        return [(ref, 0, count) for ref in refs]
    parts = [(refs[0], 0, count), (refs[0], count, count)]
    for ref in refs[1:]:
        parts += [(ref, count, count), (ref, 0, count)]
    return parts


def gather_rows(parts, slots):
    for k, (ref, top, count) in enumerate(parts):
        slots[k * count : (k + 1) * count, :] = ref[top : top + count, :].astype(F32)
    return slots[...].astype(BF16)


def mix_next(n_chip, group, layer, *refs):
    parts, (crossed, sent, slots) = slot_parts(refs[:n_chip], group), refs[n_chip:]
    facing = [parts[k ^ (group - 1)] for k in range(len(parts))]
    rows = gather_rows(facing, slots)
    sent[...] = jnp.dot(rows, crossed[layer], preferred_element_type=F32).astype(BF16)


def own_next(n_chip, group, layer, *refs):
    parts, (weight, base, held, slots) = slot_parts(refs[:n_chip], group), refs[n_chip:]
    rows = gather_rows(parts, slots)
    held[...] = base[...].astype(F32) + jnp.dot(rows, weight[layer], preferred_element_type=F32)


def mix_last(n_chip, group, layer, *refs):
    parts, (crossed, order) = slot_parts(refs[:n_chip], group), refs[n_chip : n_chip + 2]
    outs, slots = refs[n_chip + 2 : -1], refs[-1]
    rows = outs[0].shape[0]
    moved = jnp.dot(order[...], gather_rows(parts, slots), preferred_element_type=F32)
    product = jnp.dot(moved.astype(BF16), crossed[layer], preferred_element_type=F32)
    for k, out in enumerate(outs):
        out[...] = product[(k + 1) * rows : (k + 2) * rows].astype(BF16)


def own_last(n_chip, group, layer, *refs):
    parts, (weight, base, order, own, slots) = slot_parts(refs[:n_chip], group), refs[n_chip:]
    rows = own.shape[0]
    moved = jnp.dot(order[...], gather_rows(parts, slots), preferred_element_type=F32)
    own[...] = jnp.dot(moved.astype(BF16), weight[layer], preferred_element_type=F32)[
        :rows
    ] + jnp.dot(order[:rows, :], base[...], preferred_element_type=F32)


def close(own, *refs):
    total = own[...]
    for part in refs[:-1]:
        total = total + part[...].astype(F32)
    refs[-1][...] = total.astype(BF16)


def in_vmem(array):
    return pltpu.with_memory_space_constraint(array, pltpu.VMEM)


def stage(n_tp, n_dp, order_in, order_out):
    total = order_in.shape[0]

    def held(dim, n, index):
        row = lax.broadcasted_iota(jnp.int32, (total, total), dim)
        size = total // n
        return peer_of(n, row // size, index) * size + row % size

    tp, dp = lax.axis_index("tp"), lax.axis_index("dp")
    order_in[...] = jnp.where(held(0, n_dp, dp) == held(1, n_tp, tp), 1.0, 0.0).astype(BF16)
    order_out[...] = jnp.where(held(0, n_tp, tp) == held(1, n_dp, dp), 1.0, 0.0).astype(BF16)


def call(body, args, in_specs, outs, scratch=(), flops=None):
    return pl.pallas_call(
        body,
        out_shape=[pltpu.VMEM(shape, dtype) for shape, dtype in outs],
        in_specs=in_specs,
        out_specs=[VMEM] * len(outs),
        scratch_shapes=[pltpu.VMEM(shape, dtype) for shape, dtype in scratch],
        compiler_params=pltpu.CompilerParams(vmem_limit_bytes=8 << 20),
        cost_estimate=flops and pl.CostEstimate(flops=flops, bytes_accessed=0, transcendentals=0),
    )(*map(in_vmem, args))


def per_device(
    n_tp,
    n_dp,
    tokens,
    norm_gain,
    w_query,
    w_forget,
    w_value,
    w_gate,
    lower_bound,
    head_gain,
    w_out,
    state,
):
    seqs, heads, hd = state.shape[1], state.shape[2], state.shape[3]
    rows, local = tokens.shape
    features = local * n_dp
    total = rows * n_tp
    width = heads * hd
    weights = (w_query, w_forget, w_value, w_gate)
    order_in, order_out = call(
        functools.partial(stage, n_tp, n_dp),
        (),
        [],
        [((total, total), BF16)] * 2,
        flops=20_000_000_000,
    )
    parts = gather("a", "tp", n_tp, tokens)
    flip = core_flip(n_dp)
    group, n_chip = flip + 1, n_dp // (flip + 1)
    crossed = cross_copy(n_dp, w_out)
    states = []
    for layer in range(2):
        (narrowed,) = call(
            functools.partial(narrow, layer), (state,), [VMEM], [(state.shape[1:], BF16)]
        )
        states.append([narrowed] + [cross_copy(n_dp, narrowed)] * flip)
    base = held = None
    new_state = None
    for layer in range(2):
        message = (group * seqs, 4 * width + LANES)
        outs = [((total, local), BF16), (message, F32)] + [(message, BF16)] * (n_dp - 1)
        specs = [VMEM] * 4
        if layer == 0:
            base, own, *sent = call(
                functools.partial(project_first, n_tp, layer),
                (*parts, order_in, norm_gain, *weights),
                [VMEM] * (n_tp + 2) + specs,
                outs,
                [((total, local), F32)],
            )
        else:
            base, own, *sent = call(
                functools.partial(project_next, n_tp, layer),
                (held, *parts, norm_gain, *weights),
                [VMEM] * (n_tp + 1) + specs,
                outs,
            )
        parts = exchange("eb"[layer == 0], "dp", n_dp, sent)
        normed, gates = call(
            functools.partial(recur, n_dp, layer, features, group),
            (own, *parts, lower_bound, head_gain, *states[layer]),
            [VMEM] * (n_dp + 2 + group),
            [((group * seqs, width), BF16), ((seqs, 3, width), F32)],
            [((4 * group * seqs, group * seqs * hd), F32)],
        )
        read = gather("fc"[layer == 0], "dp", n_dp, normed, chip_rounds(n_dp))
        slots = [((total, width), F32)]
        new_state = pl.pallas_call(
            functools.partial(update, layer),
            name="update",
            out_shape=jax.ShapeDtypeStruct(state.shape, F32),
            in_specs=[VMEM, VMEM] + ([ANY] if layer else []),
            out_specs=ANY,
            input_output_aliases={2: 0} if layer else {},
            scratch_shapes=[
                pltpu.VMEM((seqs, heads, hd, hd), F32),
                pltpu.SemaphoreType.DMA((seqs,)),
            ],
            compiler_params=pltpu.CompilerParams(vmem_limit_bytes=4 << 20),
        )(in_vmem(gates), in_vmem(state), *((new_state,) if layer else ()))
        if layer == 0:
            (sent,) = call(
                functools.partial(mix_next, n_chip, group, layer),
                (*read, crossed),
                [VMEM] * (n_chip + 1),
                [((total, local), BF16)],
                slots,
            )
            parts = cross_exchange("d", n_tp, n_dp, [sent] * (n_tp - 1))
            (held,) = call(
                functools.partial(own_next, n_chip, group, layer),
                (*read, w_out, base),
                [VMEM] * (n_chip + 2),
                [((total, local), F32)],
                slots,
            )
        else:
            sent = call(
                functools.partial(mix_last, n_chip, group, layer),
                (*read, crossed, order_out),
                [VMEM] * (n_chip + 2),
                [((rows, local), BF16)] * (n_tp - 1),
                slots,
            )
            parts = cross_exchange("g", n_tp, n_dp, sent)
            (own,) = call(
                functools.partial(own_last, n_chip, group, layer),
                (*read, w_out, base, order_out),
                [VMEM] * (n_chip + 3),
                [((rows, local), F32)],
                slots,
            )
    hidden = pl.pallas_call(
        close,
        name="close",
        out_shape=jax.ShapeDtypeStruct((rows, local), BF16),
        in_specs=[VMEM] * n_tp,
        out_specs=VMEM,
        compiler_params=pltpu.CompilerParams(vmem_limit_bytes=4 << 20),
    )(*map(in_vmem, (own, *parts)))
    return (hidden, new_state)


def solution(mesh):
    n_tp, n_dp = mesh.shape["tp"], mesh.shape["dp"]

    def body(*args):
        return per_device(n_tp, n_dp, *args)

    return jax.shard_map(
        body,
        mesh=mesh,
        in_specs=(
            P(("grp", "tp"), "dp"),
            P(None, "dp"),
            P(None, "dp", "tp"),
            P(None, "dp", "tp"),
            P(None, "dp", "tp"),
            P(None, "dp", "tp"),
            P(None, "tp"),
            P(),
            P(None, "tp", "dp"),
            P(None, ("grp", "dp"), "tp", None, None),
        ),
        out_specs=(P(("grp", "tp"), "dp"), P(None, ("grp", "dp"), "tp", None, None)),
        check_vma=False,
    )
```
